128 devices in a mesh: ep: 32 (over z, y, core), tp: 4 (over x).
Axes of the slice: x: 4, y: 4, z: 4, core: 2. Of those that a mesh axis runs over, the one named last changes fastest.
Arguments:
- query: bfloat16 [32768, 1024], P('ep', 'tp'), may hold values from -6 to 6
- keys: bfloat16 [32768, 1024], P('ep', 'tp'), may hold values from -6 to 6
- values: bfloat16 [32768, 2048], P('ep', 'tp'), may hold values from -6 to 6
- gate_pre: bfloat16 [32768, 2048], P('ep', 'tp'), may hold values from -6 to 6
- log_decay: float32 [16, 32768], P('tp', 'ep'), may hold values from -1 to 0
- out_weight: bfloat16 [2048, 4096], P(None, 'tp'), may hold values from -0.125 to 0.125
- expert_input: bfloat16 [8192, 4096], P(('ep', 'tp')), may hold values from -6 to 6
- norm_gain: float32 [4096], replicated, may hold values from 0.1 to 1.9
- routes: int32 [8192, 2], P(('ep', 'tp')), may hold values from 0 to 31, all different within a row; in each aligned block of 64 rows (0 to 63, 64 to 127, ...) at most 6 rows name the same one
- route_weights: float32 [8192, 2], P(('ep', 'tp')), may hold values from 0.1 to 1
- w_gate: bfloat16 [32, 4096, 1536], P('ep', None, 'tp'), may hold values from -0.09375 to 0.09375
- w_up: bfloat16 [32, 4096, 1536], P('ep', None, 'tp'), may hold values from -0.09375 to 0.09375
- w_down: bfloat16 [32, 1536, 4096], P('ep', 'tp'), may hold values from -0.15625 to 0.15625
Outputs:
- mixed: bfloat16 [32768, 4096], P('ep', 'tp')
- moe_out: bfloat16 [8192, 4096], P(('ep', 'tp'))
The draws below stay inside these ranges and needn't reach their ends.
Inputs may be any that keep to these rules, and one draw needn't show every extreme that they name: `routes`: each row names 2 different experts; among the rows of one device no expert is named by more than 6 rows, a bound that some block reaches of some device.
All inputs are finite; a program needn't handle non-finite values.
Results may differ from the reference program's by a relative error of at most 0.018.
Values may be sent and summed in bfloat16 or wider, within the bound.
No kernel may reach another device: no remote copies, remote signals or barrier semaphores. Data moves between devices by JAX's collectives and lax.ppermute only.
A program may use at most 128 MiB of HBM per device.

```python
import math
import jax
import jax.numpy as jnp
import numpy as np
from jax import lax

D = 4096
RETENTION_HEADS = 16
DK = 64
DV = 128
FFE = 1536
TOP = 2
BLK = 128
TB_DEV = 64
EXPERTS = 32
CAP = 6
ROWS_A = 1024
FIRST_TOKENS = 32768
TOKENS_B = 8192
N_EP = 32
N_TP = 4


def draw_log_decay(key, part):
    key_sequence = jax.random.split(jax.random.fold_in(key, 71), 7)
    fast_share = 0.5
    fast_heads = jax.random.uniform(key_sequence[0], (RETENTION_HEADS,), jnp.float32) < fast_share
    fast_rate = jnp.exp(jax.random.uniform(key_sequence[1], (RETENTION_HEADS,), jnp.float32, jnp.log(1.0 / 80.0), jnp.log(1.0 / 30.0)))
    slow_rate = jax.random.uniform(key_sequence[2], (RETENTION_HEADS,), jnp.float32, 0.3, 0.8) / FIRST_TOKENS
    base_rate = jnp.where(fast_heads, fast_rate, slow_rate)
    span_len = max(ROWS_A // 2, 1)
    span_count = FIRST_TOKENS // span_len
    span_factor = jnp.exp(jax.random.uniform(key_sequence[3], (RETENTION_HEADS, span_count), jnp.float32, jnp.log(0.4), jnp.log(2.5)))
    span_factor = jnp.repeat(span_factor, span_len, axis=1)
    roughness = jnp.exp(jax.random.uniform(key_sequence[4], (RETENTION_HEADS, FIRST_TOKENS), jnp.float32, -0.5, 0.5))
    logarithm_rate = -(base_rate[:, None] * span_factor * roughness)
    spike_position = jax.random.randint(key_sequence[5], (3,), 0, FIRST_TOKENS)
    spike_strength = jnp.log(jax.random.uniform(key_sequence[6], (RETENTION_HEADS, 3), jnp.float32, 0.5, 0.8))
    position_index = jnp.arange(FIRST_TOKENS, dtype=jnp.int32)
    expert_hits = (position_index[None, :] == spike_position[:, None]).astype(jnp.float32)
    decay_spikes = jnp.dot(spike_strength, expert_hits)
    return (logarithm_rate + decay_spikes).astype(jnp.float32)


def steps_of(key, extent, cuts, low, high):
    gain, own = 1.0, jax.random.fold_in(key, 6)
    for axis_at, blocks in cuts:
        steps = jnp.exp(jax.random.uniform(jax.random.fold_in(own, axis_at), (blocks,), jnp.float32, low / len(cuts), high / len(cuts)))
        gain = gain * jnp.repeat(steps, extent[axis_at] // blocks).reshape([-1 if axis == axis_at else 1 for axis in range(len(extent))])
    return gain


def deal_out(stream_key, own, number, rows, count, top, most, slope):
    order = jax.random.permutation(stream_key, count)
    crowded, common = portions_of(count, rows * top, most, slope, True), portions_of(count, rows * top, most, slope, False)
    places = jnp.arange(count)

    def named(tallies, offset_by):
        used = int((tallies > 0).sum())
        fixed = max(1, used // 4)
        passed = fixed + (places - fixed + offset_by * (used - fixed)) % max(1, count - fixed)
        return jnp.zeros((count,), jnp.int32).at[order[jnp.where(places < fixed, places, passed)]].set(jnp.asarray(tallies, jnp.int32))

    tallies = jnp.where(number % 4 == 0, named(crowded, number // 4), named(common, number - number // 4 - 1))
    mixed = jax.random.permutation(jax.random.fold_in(own, 3), count)
    donor, sink = mixed[0:count // 2 * 2:2], mixed[1:count // 2 * 2:2]
    slack = jnp.minimum(tallies[donor] - 1, most - tallies[sink]) // 2
    slack = jnp.where((donor == order[0]) | (sink == order[0]) | (tallies[sink] == 0), 0, jnp.maximum(slack, 0))
    passed = jax.random.randint(jax.random.fold_in(own, 4), (count // 2,), 0, 1 << 20) % (slack + 1)
    tallies = tallies.at[donor].add(-passed).at[sink].add(passed)
    items = jnp.searchsorted(jnp.cumsum(tallies), jnp.arange(rows * top), side="right").astype(jnp.int32)
    listing = items.reshape(top, rows).T
    listing = listing[jax.random.permutation(jax.random.fold_in(own, 1), rows)]
    offset_by = jax.random.randint(jax.random.fold_in(own, 2), (rows, 1), 0, top)
    return jnp.take_along_axis(listing, (jnp.arange(top)[None, :] + offset_by) % top, axis=1)


def portions_of(number_of, total, bound, lean, full):
    weights = [(1 << 20) // math.isqrt(rank ** lean) + 1 for rank in range(1, number_of + 1)]
    largest = bound if full else min(bound, max(-(-total // number_of), total * weights[0] // sum(weights)))
    least = 1 if total - largest >= number_of - 1 else 0
    given, surplus = [largest] + [least] * (number_of - 1), total - largest - least * (number_of - 1)
    while surplus > 0:
        candidates = [i for i in range(1, number_of) if given[i] < largest] or [i for i in range(1, number_of) if given[i] < bound]
        whole, left = sum([weights[i] for i in candidates]), surplus
        for i in candidates:
            more = min(bound - given[i], max(1, left * weights[i] // whole), surplus)
            given[i] = given[i] + more
            surplus = surplus - more
    return np.array(given)


def noise(rng, shape, deviation, reach, cuts=(), kind=jnp.bfloat16):
    factor_of = steps_of(rng, shape, cuts, -0.22, 0.18) if cuts else 1.0
    values = jax.random.normal(rng, shape, jnp.float32) * deviation * factor_of
    return jnp.minimum(jnp.maximum(values, -reach), reach).astype(kind)


def setup_inputs(seed: int = 0) -> dict:
    arg_keys = jax.random.split(jax.random.key(seed), 14)
    query = noise(arg_keys[0], (FIRST_TOKENS, RETENTION_HEADS * DK), 1.0, 6.0, ((0, 32), (1, 4)))
    keys = noise(arg_keys[1], (FIRST_TOKENS, RETENTION_HEADS * DK), 1.0, 6.0, ((0, 32), (1, 4)))
    values = noise(arg_keys[2], (FIRST_TOKENS, RETENTION_HEADS * DV), 1.0, 6.0, ((0, 32), (1, 4)))
    gate_pre = noise(arg_keys[3], (FIRST_TOKENS, RETENTION_HEADS * DV), 1.0, 6.0, ((0, 32), (1, 4)))
    log_decay = draw_log_decay(jax.random.fold_in(arg_keys[13], 71), 0)
    out_weight = noise(arg_keys[5], (RETENTION_HEADS * DV, D), (RETENTION_HEADS * DV) ** -0.5, 0.125, ((1, 4),))
    expert_input = noise(arg_keys[6], (TOKENS_B, D), 1.0, 6.0, ((0, 128),))
    norm_gain = jnp.clip(1.0 + 0.18 * jax.random.normal(arg_keys[7], (D,), jnp.float32), 0.1, 1.9)
    routes_keys = jax.random.split(jax.random.fold_in(arg_keys[8], 1), TOKENS_B // TB_DEV)
    routes_turns = jax.random.permutation(jax.random.fold_in(arg_keys[8], 3), TOKENS_B // TB_DEV)
    routes = jax.vmap(lambda own, number: deal_out(jax.random.fold_in(arg_keys[8], 2), own, number, TB_DEV, EXPERTS, TOP, CAP, 1))(routes_keys, routes_turns).reshape((TOKENS_B, TOP))
    route_weights = jnp.clip(0.1 + 0.9 * jax.random.uniform(arg_keys[9], (TOKENS_B, TOP), jnp.float32) ** steps_of(arg_keys[9], (TOKENS_B, TOP), ((0, 128),), -0.2, 0.2), 0.1, 1.0)
    w_gate = noise(arg_keys[10], (EXPERTS, D, FFE), D ** -0.5, 0.09375, ((0, 32), (2, 4)))
    w_up = noise(arg_keys[11], (EXPERTS, D, FFE), D ** -0.5, 0.09375, ((0, 32), (2, 4)))
    w_down = noise(arg_keys[12], (EXPERTS, FFE, D), FFE ** -0.5, 0.15625, ((0, 32), (1, 4)))
    return {"query": query, "keys": keys, "values": values, "gate_pre": gate_pre, "log_decay": log_decay, "out_weight": out_weight, "expert_input": expert_input, "norm_gain": norm_gain, "routes": routes, "route_weights": route_weights, "w_gate": w_gate, "w_up": w_up, "w_down": w_down}


def rotate(vectors, position_index):
    half_dim = vectors.shape[-1] // 2
    inverse = 1.0 / 10000.0 ** jnp.linspace(0.0, 1.0, half_dim, dtype=jnp.float32)
    angles = position_index[:, None] * inverse[None, :]
    cosine = jnp.cos(angles)[:, None, :]
    sine_part = jnp.sin(angles)[:, None, :]
    first_half = vectors[..., :half_dim]
    second_half = vectors[..., half_dim:]
    return jnp.concatenate([first_half * cosine - second_half * sine_part, first_half * sine_part + second_half * cosine], axis=-1)

def retention_block(state, inputs):
    query_blk, key_blk, value_blk, decay_blk = inputs
    width_blk = decay_blk.shape[1]
    running = jnp.cumsum(decay_blk, axis=1)
    spread = running[:, :, None] - running[:, None, :]
    causal = jnp.tril(jnp.ones((width_blk, width_blk), dtype=bool))[None]
    weights = jnp.where(causal, jnp.exp(jnp.where(causal, spread, 0.0)), 0.0)
    highest = lax.Precision.HIGHEST
    scores = jnp.einsum('hid,hjd->hij', query_blk, key_blk, precision=highest) * weights
    output = jnp.einsum('hij,hje->hie', scores, value_blk, precision=highest)
    output = output + jnp.einsum('hid,hde->hie', query_blk * jnp.exp(running)[:, :, None], state, precision=highest)
    closing = running[:, -1:]
    state_next = state * jnp.exp(closing)[:, :, None] + jnp.einsum('hjd,hje->hde', key_blk * jnp.exp(closing - running)[:, :, None], value_blk, precision=highest)
    return (state_next, output)

def head_norm(vectors):
    centered = vectors - lax.optimization_barrier(jnp.mean(vectors, axis=-1, keepdims=True))
    variance = lax.optimization_barrier(jnp.mean(centered * centered, axis=-1, keepdims=True))
    return centered * lax.rsqrt(variance + 1e-06)

def mixer(query, keys, values, gate_pre, log_decay, out_weight):
    length = query.shape[0]
    position_index = jnp.arange(length, dtype=jnp.int32).astype(jnp.float32)
    rotated_q = rotate(query.astype(jnp.float32).reshape(length, RETENTION_HEADS, DK), position_index)
    rotated_k = rotate(keys.astype(jnp.float32).reshape(length, RETENTION_HEADS, DK), position_index) * DK ** (-0.5)
    value_rows = values.astype(jnp.float32).reshape(length, RETENTION_HEADS, DV)
    block_count = length // BLK

    def to_blocks(array):
        return array.reshape(block_count, BLK, RETENTION_HEADS, array.shape[-1]).transpose(0, 2, 1, 3)
    decay_blocks = log_decay.reshape(RETENTION_HEADS, block_count, BLK).transpose(1, 0, 2)
    start_state = jnp.zeros((RETENTION_HEADS, DK, DV), jnp.float32)
    final_state, outputs = lax.scan(retention_block, start_state, (to_blocks(rotated_q), to_blocks(rotated_k), to_blocks(value_rows), decay_blocks))
    combined = outputs.transpose(0, 2, 1, 3).reshape(length, RETENTION_HEADS, DV)
    gate_act = jax.nn.silu(gate_pre.astype(jnp.float32).reshape(length, RETENTION_HEADS, DV))
    gated = (gate_act * head_norm(combined)).reshape(length, RETENTION_HEADS * DV).astype(jnp.bfloat16)
    return jnp.dot(gated, out_weight, preferred_element_type=jnp.float32).astype(jnp.bfloat16)

def experts(expert_input, norm_gain, routes, route_weights, w_gate, w_up, w_down):
    rows_f = expert_input.astype(jnp.float32)
    centered = rows_f - lax.optimization_barrier(jnp.mean(rows_f, axis=-1, keepdims=True))
    variance = lax.optimization_barrier(jnp.mean(centered * centered, axis=-1, keepdims=True))
    normed = (centered * lax.rsqrt(variance + 1e-05) * norm_gain).astype(jnp.bfloat16)
    pair_count = TOKENS_B * TOP
    expert_ids = routes.reshape(pair_count).astype(jnp.int32)
    limit = N_EP * N_TP * CAP
    block_width = FFE // N_TP

    def one_expert(pair_out, index):
        chosen = jnp.nonzero(expert_ids == index, size=limit, fill_value=pair_count)[0].astype(jnp.int32)
        token_rows = jnp.minimum(chosen // TOP, TOKENS_B - 1).astype(jnp.int32)
        rows_in = normed[token_rows]
        gate_w = lax.dynamic_index_in_dim(w_gate, index, 0, keepdims=False)
        up_w = lax.dynamic_index_in_dim(w_up, index, 0, keepdims=False)
        down_w = lax.dynamic_index_in_dim(w_down, index, 0, keepdims=False)
        hidden = (jax.nn.silu(jnp.dot(rows_in, gate_w, preferred_element_type=jnp.float32)) * jnp.dot(rows_in, up_w, preferred_element_type=jnp.float32)).astype(jnp.bfloat16)
        total = jnp.zeros((limit, D), jnp.float32)
        for part_index in range(N_TP):
            lower = part_index * block_width
            part_rows = jnp.dot(hidden[:, lower:lower + block_width], down_w[lower:lower + block_width], preferred_element_type=jnp.float32).astype(jnp.bfloat16)
            total = total + lax.optimization_barrier(part_rows).astype(jnp.float32)
        pair_out = pair_out.at[chosen].set(total.astype(jnp.bfloat16), mode='drop')
        return (pair_out, None)
    pair_out, _ = lax.scan(one_expert, jnp.zeros((pair_count, D), jnp.bfloat16), jnp.arange(EXPERTS, dtype=jnp.int32))
    weighted = pair_out.reshape(TOKENS_B, TOP, D).astype(jnp.float32) * route_weights[:, :, None]
    return lax.optimization_barrier(jnp.sum(weighted, axis=1)).astype(jnp.bfloat16)

def reference(query, keys, values, gate_pre, log_decay, out_weight, expert_input, norm_gain, routes, route_weights, w_gate, w_up, w_down):
    mixed = mixer(query, keys, values, gate_pre, log_decay, out_weight)
    moe_out = experts(expert_input, norm_gain, routes, route_weights, w_gate, w_up, w_down)
    return (mixed, moe_out)
```

```python
import jax
import jax.numpy as jnp
from jax import lax
from jax.experimental import pallas as pl
from jax.experimental.pallas import tpu as pltpu
from jax.sharding import Mesh
from jax.sharding import PartitionSpec as P


EP = ("ep_0", "ep_1", "ep_2")
EP_TP = ("ep_0", "ep_1", "ep_2", "tp")
CHUNK = 256
META = 128
ROW = 8
D_B = 1280
R_B = 1280
F32 = jnp.float32
BF16 = jnp.bfloat16


def send(value, axis, step):
    n = lax.axis_size(axis)
    return lax.ppermute(value, axis, [(i, (i + step) % n) for i in range(n)])


def after(value, *earlier):
    return lax.optimization_barrier((value, earlier))[0]


def mm(a, b):
    return jnp.dot(a, b, preferred_element_type=F32)


def mm_t(a, b):
    return lax.dot_general(a, b, (((0,), (0,)), ((), ())), preferred_element_type=F32)


def turned(x, cosine, sine):
    lane = lax.broadcasted_iota(jnp.int32, x.shape, 1) % 64
    other = jnp.where(lane < 32, pltpu.roll(x, 96, 1), pltpu.roll(x, 32, 1))
    return x * cosine + other * sine


def state_kernel(k_ref, v_ref, cos_ref, sin_ref, cum_t_ref, out_ref, state_ref):
    step = pl.program_id(0)
    heads = v_ref.shape[1] // 128

    @pl.when(step == 0)
    def _():
        state_ref[...] = jnp.zeros_like(state_ref)

    cosine = cos_ref[...]
    sine = sin_ref[...]
    half = lax.broadcasted_iota(jnp.int32, (CHUNK, 128), 1) < 64
    for pair in range(heads // 2):
        lanes = slice(128 * pair, 128 * pair + 128)
        k = turned(k_ref[:, lanes].astype(F32), cosine, sine) * 0.125
        c0 = cum_t_ref[:, 2 * pair : 2 * pair + 1]
        c1 = cum_t_ref[:, 2 * pair + 1 : 2 * pair + 2]
        t0 = c0[CHUNK - 1 : CHUNK, :]
        t1 = c1[CHUNK - 1 : CHUNK, :]
        k = k * jnp.exp(jnp.where(half, t0 - c0, t1 - c1))
        v = v_ref[:, 256 * pair : 256 * pair + 256]
        new = mm_t(k.astype(BF16), v)
        for j, t in ((0, t0), (1, t1)):
            h = 2 * pair + j
            rows = slice(64 * h, 64 * h + 64)
            state_ref[rows, :] = (
                state_ref[rows, :] * jnp.exp(t) + new[64 * j : 64 * j + 64, 128 * j : 128 * j + 128]
            )

    @pl.when(step == pl.num_programs(0) - 1)
    def _():
        out_ref[...] = state_ref[...]


def output_kernel(
    q_ref, k_ref, v_ref, g_ref, cos_ref, sin_ref, cum_ref, cum_t_ref, inc_ref, out_ref, state_ref
):
    step = pl.program_id(0)
    heads = v_ref.shape[1] // 128

    @pl.when(step == 0)
    def _():
        state_ref[...] = jnp.zeros_like(state_ref)
        for h in range(heads):
            low = 64 * (h % 2)
            state_ref[h, low : low + 64, :] = inc_ref[64 * h : 64 * h + 64, :]

    cosine = cos_ref[...]
    sine = sin_ref[...]
    half = lax.broadcasted_iota(jnp.int32, (CHUNK, 128), 1) < 64
    causal = lax.broadcasted_iota(jnp.int32, (CHUNK, CHUNK), 0) >= lax.broadcasted_iota(
        jnp.int32, (CHUNK, CHUNK), 1
    )
    for pair in range(heads // 2):
        lanes = slice(128 * pair, 128 * pair + 128)
        q = turned(q_ref[:, lanes].astype(F32), cosine, sine)
        k = turned(k_ref[:, lanes].astype(F32), cosine, sine) * 0.125
        k_b = k.astype(BF16)
        for j in range(2):
            h = 2 * pair + j
            mine = half if j == 0 else jnp.logical_not(half)
            v = v_ref[:, 128 * h : 128 * h + 128]
            col = cum_t_ref[:, h : h + 1]
            row = cum_ref[0, h : h + 1, :]
            total = col[CHUNK - 1 : CHUNK, :]
            q_h = jnp.where(mine, q, 0.0)
            weights = jnp.exp(jnp.where(causal, col - row, -1e9))
            scores = (
                lax.dot_general(
                    q_h.astype(BF16), k_b, (((1,), (1,)), ((), ())), preferred_element_type=F32
                )
                * weights
            )
            state = state_ref[h]
            out = mm(scores.astype(BF16), v) + mm(
                (q_h * jnp.exp(col)).astype(BF16), state.astype(BF16)
            )
            k_h = jnp.where(mine, k * jnp.exp(total - col), 0.0)
            state_ref[h] = state * jnp.exp(total) + mm_t(k_h.astype(BF16), v)
            centered = out - jnp.mean(out, axis=1, keepdims=True)
            variance = jnp.mean(centered * centered, axis=1, keepdims=True)
            normed = centered * lax.rsqrt(variance + 1e-06)
            gate = g_ref[:, 128 * h : 128 * h + 128].astype(F32)
            out_ref[:, 128 * h : 128 * h + 128] = (gate * jax.nn.sigmoid(gate) * normed).astype(
                BF16
            )


def local_state(keys, values, cosine, sine, cum_t):
    rows, width = keys.shape
    grid = rows // CHUNK
    heads = values.shape[1] // 128
    return pl.pallas_call(
        state_kernel,
        name="local_state",
        grid=(grid,),
        in_specs=[
            pl.BlockSpec((CHUNK, width), lambda i: (i, 0)),
            pl.BlockSpec((CHUNK, values.shape[1]), lambda i: (i, 0)),
            pl.BlockSpec((CHUNK, 128), lambda i: (i, 0)),
            pl.BlockSpec((CHUNK, 128), lambda i: (i, 0)),
            pl.BlockSpec((CHUNK, heads), lambda i: (i, 0)),
        ],
        out_specs=pl.BlockSpec((64 * heads, 128), lambda i: (0, 0)),
        out_shape=jax.ShapeDtypeStruct((64 * heads, 128), F32),
        scratch_shapes=[pltpu.VMEM((64 * heads, 128), F32)],
        cost_estimate=pl.CostEstimate(
            flops=2 * rows * width * 256, bytes_accessed=3 << 20, transcendentals=1 << 18
        ),
    )(keys, values, cosine, sine, cum_t)


def gated_output(query, keys, values, gate_pre, cosine, sine, cum, cum_t, incoming):
    rows, width = keys.shape
    grid = rows // CHUNK
    vw = values.shape[1]
    heads = vw // 128
    return pl.pallas_call(
        output_kernel,
        name="gated_output",
        grid=(grid,),
        in_specs=[
            pl.BlockSpec((CHUNK, width), lambda i: (i, 0)),
            pl.BlockSpec((CHUNK, width), lambda i: (i, 0)),
            pl.BlockSpec((CHUNK, vw), lambda i: (i, 0)),
            pl.BlockSpec((CHUNK, vw), lambda i: (i, 0)),
            pl.BlockSpec((CHUNK, 128), lambda i: (i, 0)),
            pl.BlockSpec((CHUNK, 128), lambda i: (i, 0)),
            pl.BlockSpec((1, heads, CHUNK), lambda i: (i, 0, 0)),
            pl.BlockSpec((CHUNK, heads), lambda i: (i, 0)),
            pl.BlockSpec((64 * heads, 128), lambda i: (0, 0)),
        ],
        out_specs=pl.BlockSpec((CHUNK, vw), lambda i: (i, 0)),
        out_shape=jax.ShapeDtypeStruct((rows, vw), BF16),
        scratch_shapes=[pltpu.VMEM((heads, 128, 128), F32)],
        cost_estimate=pl.CostEstimate(
            flops=10 * 1000 * 1000 * 1000, bytes_accessed=5 << 20, transcendentals=1 << 20
        ),
    )(query, keys, values, gate_pre, cosine, sine, cum, cum_t, incoming)


def pack_state(state, log_total):
    high = log_total.astype(BF16)
    low = (log_total - high.astype(F32)).astype(BF16)
    extra = jnp.concatenate([high[:, None], low[:, None]], axis=0)
    extra = jnp.broadcast_to(extra, (extra.shape[0], 128))
    return jnp.concatenate([state.astype(BF16), extra], axis=0)


def unpack_state(packed, heads):
    state = packed[: 64 * heads].astype(F32)
    logs = packed[64 * heads :, 0].astype(F32)
    return state, logs[:heads] + logs[heads:]


def scaled(state, log_factor):
    return state * jnp.repeat(jnp.exp(log_factor), 64)[:, None]


def core_prefix(state, log_total):
    heads = log_total.shape[0]
    second = lax.axis_index("ep_2") == 1
    mine = pack_state(state, log_total)
    other_state, other_log = unpack_state(send(mine, "ep_2", 1), heads)
    state = unpack_state(mine, heads)[0]
    inside = (jnp.where(second, other_state, 0.0), jnp.where(second, other_log, 0.0))
    first_s = jnp.where(second, other_state, state)
    second_s = jnp.where(second, state, other_state)
    second_log = jnp.where(second, log_total, other_log)
    group = pack_state(scaled(first_s, second_log) + second_s, log_total + other_log)
    return inside, group


def ring_prefix(inside, packed, axis, heads):
    count = lax.axis_size(axis)
    position = lax.axis_index(axis)
    pieces = [unpack_state(packed, heads)] + [
        unpack_state(send(packed, axis, d), heads) for d in range(1, count)
    ]
    places = [(position - d) % count for d in range(count)]
    before = jnp.zeros_like(pieces[0][0])
    before_log = jnp.zeros_like(pieces[0][1])
    for d in range(1, count):
        ok = position >= d
        before = before + jnp.where(ok, scaled(pieces[d][0], before_log), 0.0)
        before_log = before_log + jnp.where(ok, pieces[d][1], 0.0)
    inside = (scaled(before, inside[1]) + inside[0], inside[1] + before_log)
    group_state = jnp.zeros_like(before)
    for d in range(count):
        later = jnp.zeros_like(before_log)
        for k in range(count):
            if k != d:
                later = later + jnp.where(places[k] > places[d], pieces[k][1], 0.0)
        group_state = group_state + scaled(pieces[d][0], later)
    return inside, pack_state(group_state, sum(piece[1] for piece in pieces))


def tables(rows):
    offset = lax.axis_index(EP) * rows
    position = (offset + jnp.arange(rows, dtype=jnp.int32)).astype(F32)
    inverse = 1.0 / 10000.0 ** jnp.linspace(0.0, 1.0, 32, dtype=F32)
    angles = position[:, None] * jnp.tile(inverse, 4)[None, :]
    sign = jnp.where(jnp.arange(128) % 64 < 32, -1.0, 1.0).astype(F32)
    return jnp.cos(angles), jnp.sin(angles) * sign[None, :]


def running(log_decay):
    heads, rows = log_decay.shape
    chunks = rows // CHUNK
    upper = (jnp.arange(CHUNK)[:, None] <= jnp.arange(CHUNK)[None, :]).astype(F32)
    cum = jnp.dot(
        log_decay.reshape(heads * chunks, CHUNK), upper, precision=lax.Precision.HIGHEST
    ).reshape(heads, chunks, CHUNK)
    return cum.transpose(1, 0, 2), cum.transpose(1, 2, 0).reshape(rows, heads)


def ring_first(value):
    return send(value, "tp", 1), send(value, "tp", -1)


def ring_second(left, right, *earlier):
    half = left.shape[0] // 2
    top, bottom = after(left[:half], *earlier), after(right[half:], *earlier)
    top = send(top, "tp", 1)
    bottom = send(bottom, "tp", -1)
    return [top, bottom]


def weight_part(out_weight, d):
    height = out_weight.shape[0] // 4
    start = (lax.axis_index("tp") - d) % 4 * height
    return lax.dynamic_slice_in_dim(out_weight, start, height, axis=0)


def token_kernel(x_ref, gain_ref, routes_ref, weights_ref, a_ref, b_ref, meta_ref, *, capacity):
    tokens, width = x_ref.shape
    x = x_ref[...].astype(F32)
    centered = x - jnp.mean(x, axis=1, keepdims=True)
    variance = jnp.mean(centered * centered, axis=1, keepdims=True)
    normed = (centered * lax.rsqrt(variance + 1e-05) * gain_ref[...]).astype(BF16)
    first = routes_ref[0:1, :]
    second = routes_ref[1:2, :]
    expert = lax.broadcasted_iota(jnp.int32, (32, tokens), 0)
    hit_0 = (expert == first).astype(F32)
    hit_1 = (expert == second).astype(F32)
    sooner = lax.broadcasted_iota(jnp.int32, (tokens, tokens), 0) < lax.broadcasted_iota(
        jnp.int32, (tokens, tokens), 1
    )
    earlier = mm((hit_0 + hit_1).astype(BF16), sooner.astype(F32).astype(BF16))
    slot_0 = jnp.sum(earlier * hit_0, axis=0, keepdims=True)
    slot_1 = jnp.sum(earlier * hit_1, axis=0, keepdims=True)
    first_f = first.astype(F32)
    second_f = second.astype(F32)
    row_0 = first_f * ROW + slot_0
    row_1 = second_f * ROW + slot_1
    line = lax.broadcasted_iota(jnp.int32, (8, tokens), 0)
    facts = jnp.zeros((8, tokens), F32)
    for index, row in enumerate(
        (
            first_f * capacity + slot_0,
            second_f * capacity + slot_1,
            weights_ref[0:1, :],
            weights_ref[1:2, :],
            row_0,
            row_1,
        )
    ):
        facts = jnp.where(line == index, row, facts)
    spot = lax.broadcasted_iota(jnp.int32, (8, META), 0) == lax.broadcasted_iota(
        jnp.int32, (8, META), 1
    )
    meta = mm_t(facts.astype(BF16), spot.astype(F32).astype(BF16))
    meta_ref[...] = meta
    place = lax.broadcasted_iota(jnp.int32, (a_ref.shape[0], tokens), 0)
    chosen = jnp.logical_or(
        place == row_0.astype(jnp.int32), place == row_1.astype(jnp.int32)
    )
    a_width = a_ref.shape[1]
    a_ref[...] = mm(chosen.astype(F32).astype(BF16), normed[:, :a_width]).astype(BF16)
    b_ref[:, : width - a_width] = normed[:, a_width:]
    b_ref[:, width - a_width :] = meta.astype(BF16)


def token_rows(expert_input, norm_gain, routes, route_weights, capacity, b_width):
    tokens, width = expert_input.shape
    kernel = lambda *refs: token_kernel(*refs, capacity=float(capacity))
    return pl.pallas_call(
        kernel,
        name="token_rows",
        out_shape=(
            jax.ShapeDtypeStruct((32 * ROW, width - b_width), BF16),
            jax.ShapeDtypeStruct((tokens, b_width + META), BF16),
            jax.ShapeDtypeStruct((tokens, META), F32),
        ),
        cost_estimate=pl.CostEstimate(
            flops=1 << 24, bytes_accessed=1 << 20, transcendentals=tokens
        ),
    )(expert_input, norm_gain[None, :], routes.T, route_weights.T)


def slot_row(target, source_x, source_core, here, capacity):
    expert = (target * 10923) >> 16
    slot = target - expert * capacity
    far = ((expert >> 3) - here[0]) & 3
    near = (((expert >> 1) & 3) - here[1]) & 3
    other = (expert - here[2]) & 1
    row = (near * 4 + far) * 8 * capacity + source_x * 2 * capacity + source_core * capacity + slot
    return jnp.where(other == 0, row, -1)


def place_kernel(here_ref, p0, p1, p2, p3, sw, o0, o1, o2, o3, meta_ref, all_ref, *, capacity):
    tokens = p0.shape[0]
    width = o0.shape[1]
    for d, p in enumerate((p0, p1, p2, p3)):
        all_ref[tokens * d : tokens * d + tokens, :] = p[...]
    all_ref[4 * tokens :, :] = sw[...]
    meta = all_ref[:, width:]
    meta_ref[...] = meta
    here = (here_ref[0], here_ref[1], here_ref[2])
    spot = lax.broadcasted_iota(jnp.int32, (8, META), 0) == lax.broadcasted_iota(
        jnp.int32, (8, META), 1
    )
    facts = lax.dot_general(
        spot.astype(F32).astype(BF16), meta, (((1,), (1,)), ((), ())), preferred_element_type=F32
    )
    token = lax.broadcasted_iota(jnp.int32, (1, 8 * tokens), 1)
    source_core = token // (4 * tokens)
    source_x = token // tokens - 4 * source_core
    rows = [
        slot_row(facts[r : r + 1, :].astype(jnp.int32), source_x, source_core, here, capacity)
        for r in range(2)
    ]
    count = o0.shape[0]
    values = all_ref[:, :width]
    for d, out in enumerate((o0, o1, o2, o3)):
        place = lax.broadcasted_iota(jnp.int32, (count, 8 * tokens), 0) + d * count
        chosen = jnp.logical_or(place == rows[0], place == rows[1])
        out[...] = mm(chosen.astype(F32).astype(BF16), values).astype(BF16)


def placed_rows(here, pieces, swapped, width, capacity):
    tokens = pieces[0].shape[0]
    count = 32 * capacity
    vmem = pl.BlockSpec(memory_space=pltpu.VMEM)
    kernel = lambda *refs: place_kernel(*refs, capacity=capacity)
    result = pl.pallas_call(
        kernel,
        name="placed_rows",
        in_specs=[pl.BlockSpec(memory_space=pltpu.SMEM)] + [vmem] * 5,
        out_specs=(vmem,) * 5,
        out_shape=(jax.ShapeDtypeStruct((count, width), BF16),) * 4
        + (jax.ShapeDtypeStruct((8 * tokens, META), BF16),),
        scratch_shapes=[pltpu.VMEM((8 * tokens, width + META), BF16)],
        cost_estimate=pl.CostEstimate(flops=1 << 30, bytes_accessed=4 << 20, transcendentals=0),
    )(here, *pieces, swapped)
    return list(result[:4]), result[4]


def regroup_kernel(i0, i1, i2, i3, o0, o1, o2, o3):
    count = i0.shape[0] // 4
    for d, out in enumerate((o0, o1, o2, o3)):
        for j, source in enumerate((i0, i1, i2, i3)):
            out[count * j : count * j + count, :] = source[count * d : count * d + count, :]


def regrouped(blocks):
    vmem = pl.BlockSpec(memory_space=pltpu.VMEM)
    shape = jax.ShapeDtypeStruct(blocks[0].shape, BF16)
    return list(
        pl.pallas_call(
            regroup_kernel,
            name="regrouped",
            in_specs=[vmem] * 4,
            out_specs=(vmem,) * 4,
            out_shape=(shape,) * 4,
            cost_estimate=pl.CostEstimate(flops=1 << 20, bytes_accessed=4 << 20, transcendentals=0),
        )(*blocks)
    )


def combine_kernel(here_ref, h0, h1, h2, h3, meta_ref, own_ref, other_ref, *, capacity):
    here = (here_ref[0], here_ref[1], here_ref[2])
    total = meta_ref.shape[0]
    token = lax.broadcasted_iota(jnp.int32, (total, 1), 0)
    source_core = token // (total // 2)
    source_x = token // (total // 8) - 4 * source_core
    meta = meta_ref[...].astype(F32)
    rows = [
        slot_row(meta[:, r : r + 1].astype(jnp.int32), source_x, source_core, here, capacity)
        for r in range(2)
    ]
    count = h0.shape[0]
    result = None
    for d, h in enumerate((h0, h1, h2, h3)):
        place = lax.broadcasted_iota(jnp.int32, (total, count), 1) + d * count
        shares = jnp.where(place == rows[0], meta[:, 2:3], 0.0) + jnp.where(
            place == rows[1], meta[:, 3:4], 0.0
        )
        product = mm(shares.astype(BF16), h[...])
        result = product if result is None else result + product
    own_ref[...] = result[: total // 2].astype(BF16)
    other_ref[...] = result[total // 2 :].astype(BF16)


def combined_rows(here, pieces, meta, capacity):
    vmem = pl.BlockSpec(memory_space=pltpu.VMEM)
    kernel = lambda *refs: combine_kernel(*refs, capacity=capacity)
    shape = jax.ShapeDtypeStruct((meta.shape[0] // 2, pieces[0].shape[1]), BF16)
    return pl.pallas_call(
        kernel,
        name="combined_rows",
        in_specs=[pl.BlockSpec(memory_space=pltpu.SMEM)] + [vmem] * 5,
        out_specs=(vmem, vmem),
        out_shape=(shape, shape),
        cost_estimate=pl.CostEstimate(flops=1 << 30, bytes_accessed=4 << 20, transcendentals=0),
    )(here, *pieces, meta)


def exchange(blocks, axis, sign):
    return [blocks[0]] + [send(blocks[d], axis, sign * d) for d in range(1, len(blocks))]


def rows_of(value, count):
    height = value.shape[0] // count
    return [value[height * d : height * (d + 1)] for d in range(count)]


def compaction(capacity):
    place = [lax.axis_index(name) for name in EP]
    index = jnp.arange(32 * capacity, dtype=jnp.int32)
    slot = index % capacity
    digits = index // capacity
    far = (place[0] - digits // 8) % 4
    near = (place[1] - digits // 2) % 4
    core = (place[2] - digits) % 2
    source = ((far * 4 + near) * 2 + core) * ROW + slot
    lanes = jnp.arange(32 * ROW, dtype=jnp.int32)
    return (source[:, None] == lanes[None, :]).astype(BF16)


def row_order(order, unit):
    count = 4**3
    index = jnp.arange(count * unit, dtype=jnp.int32)
    inside = index % unit
    digits = {}
    rest = index // unit
    for name in reversed("xzy"):
        digits[name] = rest % 4
        rest = rest // 4
    place = jnp.zeros_like(index)
    for name in order:
        place = place * 4 + digits[name]
    return place * unit + inside


def per_device(
    query,
    keys,
    values,
    gate_pre,
    log_decay,
    out_weight,
    expert_input,
    norm_gain,
    routes,
    route_weights,
    w_gate,
    w_up,
    w_down,
):
    heads = log_decay.shape[0]
    tokens, width = expert_input.shape
    top = routes.shape[1]
    capacity = 3 * tokens * top // (2 * lax.axis_size(EP))
    unit = 2 * capacity
    block = 4 * unit
    a_width = width - D_B
    gate_w, up_w, down_w = (w_gate[0], w_up[0], w_down[0])

    placed_a, payload_b, meta_a = token_rows(
        expert_input, norm_gain, routes, route_weights, capacity, D_B
    )
    here = jnp.stack([lax.axis_index(name) for name in EP]).astype(jnp.int32)
    got_b = exchange([payload_b] * 4, "tp", 1)
    got_a = lax.all_to_all(placed_a.reshape(32, ROW, a_width), EP, 0, 0, tiled=False)

    decay = after(log_decay, placed_a)
    cosine, sine = tables(query.shape[0])
    cum_c, cum_t = running(decay)
    state = local_state(keys, values, cosine, sine, cum_t)
    inside, group = core_prefix(state, jnp.sum(decay, axis=1))
    inside, group_z = ring_prefix(inside, group, "ep_1", heads)

    held_b = jnp.concatenate(after(got_b, group), axis=0)
    other_b = send(held_b, "ep_2", 1)
    blocks_b, meta_b = placed_rows(here, after(got_b, group), other_b, D_B, capacity)
    got_b = exchange(blocks_b, "ep_1", 1)
    inside, _ = ring_prefix(inside, after(group_z, blocks_b[0]), "ep_0", heads)

    compact = compaction(capacity)
    slots_a = mm(compact, after(got_a, blocks_b[0]).reshape(32 * ROW, a_width)).astype(BF16)
    left_a, right_a = ring_first(slots_a)

    gated = gated_output(
        query, keys, values, gate_pre, cosine, sine, cum_c, cum_t, after(inside[0], slots_a)
    )
    turn_b = regrouped(after(got_b, gated))
    got_b = exchange(turn_b, "ep_0", 1)
    mixed = mm(after(gated, turn_b[0]), weight_part(out_weight, 0))
    cross_a = ring_second(left_a, right_a, turn_b[0])
    left_g, right_g = ring_first(after(gated, left_a, right_a))

    all_a = jnp.concatenate(after([slots_a, left_a, *cross_a, right_a], mixed), axis=0)
    all_b = jnp.concatenate(got_b, axis=0)
    lanes = jnp.arange(16 * block, dtype=jnp.int32)
    turn = (row_order("zyx", unit)[:, None] == lanes[None, :]).astype(BF16)
    turned_b = lax.optimization_barrier(mm(turn, all_b).astype(BF16))
    gate_h = mm(all_a, gate_w[:a_width]) + mm(turned_b, gate_w[a_width:])
    up_h = mm(all_a, up_w[:a_width]) + mm(turned_b, up_w[a_width:])
    hidden = lax.optimization_barrier((jax.nn.silu(gate_h) * up_h).astype(BF16))

    ra = width - R_B
    back_a = mm(hidden, down_w[:, :ra]).astype(BF16)
    b0, b1, b2, b3 = rows_of(back_a, 4)
    half = b0.shape[0] // 2
    upper = send(b2[:half], "tp", -1)
    lower = send(b2[half:], "tp", 1)
    hidden_b = lax.optimization_barrier(mm_t(turn, after(hidden, back_a)).astype(BF16))
    back_b = mm(hidden_b, down_w[:, ra:]).astype(BF16)
    got_b = exchange(rows_of(back_b, 4), "ep_0", -1)
    mixed = mixed + mm(after(left_g, back_b), weight_part(out_weight, 1))
    b1 = jnp.concatenate([b1[:half] + after(upper, mixed), b1[half:]], axis=0)
    b3 = jnp.concatenate([b3[:half], b3[half:] + after(lower, mixed)], axis=0)
    up_a, down_a = send(b1, "tp", -1), send(b3, "tp", 1)
    cross_g = ring_second(left_g, right_g, b1, b3)
    mixed = mixed + mm(after(right_g, b1, b3), weight_part(out_weight, 3))

    turn_b = regrouped(after(got_b, mixed))
    home_b = exchange(turn_b, "ep_1", -1)
    summed_a = (
        after(b0, turn_b[0]).astype(F32) + up_a.astype(F32) + down_a.astype(F32)
    ).astype(BF16)
    spread_a = mm_t(compact, summed_a).astype(BF16)
    home_a = lax.all_to_all(
        spread_a.reshape(32, ROW, ra), EP, 0, 0, tiled=False
    ).reshape(32 * ROW, ra)
    mixed = mixed + mm(
        jnp.concatenate(after(cross_g, spread_a), axis=0), weight_part(out_weight, 2)
    )

    own_b, other_b = combined_rows(here, after(home_b, summed_a), meta_b, capacity)
    mixed_b = own_b + send(other_b, "ep_2", 1)
    final_b = sum(p.astype(F32) for p in exchange(rows_of(mixed_b, 4), "tp", -1))
    slot_lane = jnp.arange(32 * ROW, dtype=jnp.int32)[None, :]
    shares = sum(
        jnp.where(meta_a[:, 4 + r : 5 + r].astype(jnp.int32) == slot_lane, meta_a[:, 2 + r : 3 + r], 0.0)
        for r in range(top)
    ).astype(BF16)
    final_a = mm(shares, after(home_a, mixed_b))
    moe_out = jnp.concatenate([final_a, final_b], axis=1).astype(BF16)
    return (mixed.astype(BF16), moe_out)


def solution(mesh):
    torus = Mesh(mesh.devices.reshape(4, 4, 2, mesh.shape["tp"]), ("ep_0", "ep_1", "ep_2", "tp"))
    return jax.shard_map(
        per_device,
        mesh=torus,
        in_specs=(
            P(EP, "tp"),
            P(EP, "tp"),
            P(EP, "tp"),
            P(EP, "tp"),
            P("tp", EP),
            P(None, "tp"),
            P(EP_TP, None),
            P(),
            P(EP_TP, None),
            P(EP_TP, None),
            P(EP, None, "tp"),
            P(EP, None, "tp"),
            P(EP, "tp", None),
        ),
        out_specs=(P(EP, "tp"), P(EP_TP, None)),
        check_vma=False,
    )
```

```python
import jax
import jax.numpy as jnp
from jax import lax
from jax.experimental import pallas as pl
from jax.experimental.pallas import tpu as pltpu
from jax.sharding import Mesh
from jax.sharding import PartitionSpec as P


EP = ("ep_0", "ep_1", "ep_2")
EP_TP = ("ep_0", "ep_1", "ep_2", "tp")
CHUNK = 256
META = 128
ROW = 8
D_B = 1280
R_B = 1024
F32 = jnp.float32
BF16 = jnp.bfloat16


def send(value, axis, step):
    n = lax.axis_size(axis)
    return lax.ppermute(value, axis, [(i, (i + step) % n) for i in range(n)])


def after(value, *earlier):
    return lax.optimization_barrier((value, earlier))[0]


def mm(a, b):
    return jnp.dot(a, b, preferred_element_type=F32)


def mm_t(a, b):
    return lax.dot_general(a, b, (((0,), (0,)), ((), ())), preferred_element_type=F32)


def turned(x, cosine, sine):
    lane = lax.broadcasted_iota(jnp.int32, x.shape, 1) % 64
    other = jnp.where(lane < 32, pltpu.roll(x, 96, 1), pltpu.roll(x, 32, 1))
    return x * cosine + other * sine


def state_kernel(k_ref, v_ref, cos_ref, sin_ref, cum_t_ref, out_ref, state_ref):
    step = pl.program_id(0)
    heads = v_ref.shape[1] // 128

    @pl.when(step == 0)
    def _():
        state_ref[...] = jnp.zeros_like(state_ref)

    cosine = cos_ref[...]
    sine = sin_ref[...]
    half = lax.broadcasted_iota(jnp.int32, (CHUNK, 128), 1) < 64
    for pair in range(heads // 2):
        lanes = slice(128 * pair, 128 * pair + 128)
        k = turned(k_ref[:, lanes].astype(F32), cosine, sine) * 0.125
        c0 = cum_t_ref[:, 2 * pair : 2 * pair + 1]
        c1 = cum_t_ref[:, 2 * pair + 1 : 2 * pair + 2]
        t0 = c0[CHUNK - 1 : CHUNK, :]
        t1 = c1[CHUNK - 1 : CHUNK, :]
        k = k * jnp.exp(jnp.where(half, t0 - c0, t1 - c1))
        v = v_ref[:, 256 * pair : 256 * pair + 256]
        new = mm_t(k.astype(BF16), v)
        for j, t in ((0, t0), (1, t1)):
            h = 2 * pair + j
            rows = slice(64 * h, 64 * h + 64)
            state_ref[rows, :] = (
                state_ref[rows, :] * jnp.exp(t) + new[64 * j : 64 * j + 64, 128 * j : 128 * j + 128]
            )

    @pl.when(step == pl.num_programs(0) - 1)
    def _():
        out_ref[...] = state_ref[...]


def output_kernel(
    q_ref, k_ref, v_ref, g_ref, cos_ref, sin_ref, cum_ref, cum_t_ref, inc_ref, out_ref, state_ref
):
    step = pl.program_id(0)
    heads = v_ref.shape[1] // 128

    @pl.when(step == 0)
    def _():
        state_ref[...] = jnp.zeros_like(state_ref)
        for h in range(heads):
            low = 64 * (h % 2)
            state_ref[h, low : low + 64, :] = inc_ref[64 * h : 64 * h + 64, :]

    cosine = cos_ref[...]
    sine = sin_ref[...]
    half = lax.broadcasted_iota(jnp.int32, (CHUNK, 128), 1) < 64
    causal = lax.broadcasted_iota(jnp.int32, (CHUNK, CHUNK), 0) >= lax.broadcasted_iota(
        jnp.int32, (CHUNK, CHUNK), 1
    )
    for pair in range(heads // 2):
        lanes = slice(128 * pair, 128 * pair + 128)
        q = turned(q_ref[:, lanes].astype(F32), cosine, sine)
        k = turned(k_ref[:, lanes].astype(F32), cosine, sine) * 0.125
        k_b = k.astype(BF16)
        for j in range(2):
            h = 2 * pair + j
            mine = half if j == 0 else jnp.logical_not(half)
            v = v_ref[:, 128 * h : 128 * h + 128]
            col = cum_t_ref[:, h : h + 1]
            row = cum_ref[0, h : h + 1, :]
            total = col[CHUNK - 1 : CHUNK, :]
            q_h = jnp.where(mine, q, 0.0)
            weights = jnp.exp(jnp.where(causal, col - row, -1e9))
            scores = (
                lax.dot_general(
                    q_h.astype(BF16), k_b, (((1,), (1,)), ((), ())), preferred_element_type=F32
                )
                * weights
            )
            state = state_ref[h]
            out = mm(scores.astype(BF16), v) + mm(
                (q_h * jnp.exp(col)).astype(BF16), state.astype(BF16)
            )
            k_h = jnp.where(mine, k * jnp.exp(total - col), 0.0)
            state_ref[h] = state * jnp.exp(total) + mm_t(k_h.astype(BF16), v)
            centered = out - jnp.mean(out, axis=1, keepdims=True)
            variance = jnp.mean(centered * centered, axis=1, keepdims=True)
            normed = centered * lax.rsqrt(variance + 1e-06)
            gate = g_ref[:, 128 * h : 128 * h + 128].astype(F32)
            out_ref[:, 128 * h : 128 * h + 128] = (gate * jax.nn.sigmoid(gate) * normed).astype(
                BF16
            )


def local_state(keys, values, cosine, sine, cum_t):
    rows, width = keys.shape
    grid = rows // CHUNK
    heads = values.shape[1] // 128
    return pl.pallas_call(
        state_kernel,
        name="local_state",
        grid=(grid,),
        in_specs=[
            pl.BlockSpec((CHUNK, width), lambda i: (i, 0)),
            pl.BlockSpec((CHUNK, values.shape[1]), lambda i: (i, 0)),
            pl.BlockSpec((CHUNK, 128), lambda i: (i, 0)),
            pl.BlockSpec((CHUNK, 128), lambda i: (i, 0)),
            pl.BlockSpec((CHUNK, heads), lambda i: (i, 0)),
        ],
        out_specs=pl.BlockSpec((64 * heads, 128), lambda i: (0, 0)),
        out_shape=jax.ShapeDtypeStruct((64 * heads, 128), F32),
        scratch_shapes=[pltpu.VMEM((64 * heads, 128), F32)],
        cost_estimate=pl.CostEstimate(
            flops=2 * rows * width * 256, bytes_accessed=3 << 20, transcendentals=1 << 18
        ),
    )(keys, values, cosine, sine, cum_t)


def gated_output(query, keys, values, gate_pre, cosine, sine, cum, cum_t, incoming):
    rows, width = keys.shape
    grid = rows // CHUNK
    vw = values.shape[1]
    heads = vw // 128
    return pl.pallas_call(
        output_kernel,
        name="gated_output",
        grid=(grid,),
        in_specs=[
            pl.BlockSpec((CHUNK, width), lambda i: (i, 0)),
            pl.BlockSpec((CHUNK, width), lambda i: (i, 0)),
            pl.BlockSpec((CHUNK, vw), lambda i: (i, 0)),
            pl.BlockSpec((CHUNK, vw), lambda i: (i, 0)),
            pl.BlockSpec((CHUNK, 128), lambda i: (i, 0)),
            pl.BlockSpec((CHUNK, 128), lambda i: (i, 0)),
            pl.BlockSpec((1, heads, CHUNK), lambda i: (i, 0, 0)),
            pl.BlockSpec((CHUNK, heads), lambda i: (i, 0)),
            pl.BlockSpec((64 * heads, 128), lambda i: (0, 0)),
        ],
        out_specs=pl.BlockSpec((CHUNK, vw), lambda i: (i, 0)),
        out_shape=jax.ShapeDtypeStruct((rows, vw), BF16),
        scratch_shapes=[pltpu.VMEM((heads, 128, 128), F32)],
        cost_estimate=pl.CostEstimate(
            flops=10 * 1000 * 1000 * 1000, bytes_accessed=5 << 20, transcendentals=1 << 20
        ),
    )(query, keys, values, gate_pre, cosine, sine, cum, cum_t, incoming)


def pack_state(state, log_total):
    high = log_total.astype(BF16)
    low = (log_total - high.astype(F32)).astype(BF16)
    extra = jnp.concatenate([high[:, None], low[:, None]], axis=0)
    extra = jnp.broadcast_to(extra, (extra.shape[0], 128))
    return jnp.concatenate([state.astype(BF16), extra], axis=0)


def unpack_state(packed, heads):
    state = packed[: 64 * heads].astype(F32)
    logs = packed[64 * heads :, 0].astype(F32)
    return state, logs[:heads] + logs[heads:]


def scaled(state, log_factor):
    return state * jnp.repeat(jnp.exp(log_factor), 64)[:, None]


def core_prefix(state, log_total):
    heads = log_total.shape[0]
    second = lax.axis_index("ep_2") == 1
    mine = pack_state(state, log_total)
    other_state, other_log = unpack_state(send(mine, "ep_2", 1), heads)
    state = unpack_state(mine, heads)[0]
    inside = (jnp.where(second, other_state, 0.0), jnp.where(second, other_log, 0.0))
    first_s = jnp.where(second, other_state, state)
    second_s = jnp.where(second, state, other_state)
    second_log = jnp.where(second, log_total, other_log)
    group = pack_state(scaled(first_s, second_log) + second_s, log_total + other_log)
    return inside, group


def ring_prefix(inside, packed, axis, heads):
    count = lax.axis_size(axis)
    position = lax.axis_index(axis)
    pieces = [unpack_state(packed, heads)] + [
        unpack_state(send(packed, axis, d), heads) for d in range(1, count)
    ]
    places = [(position - d) % count for d in range(count)]
    before = jnp.zeros_like(pieces[0][0])
    before_log = jnp.zeros_like(pieces[0][1])
    for d in range(1, count):
        ok = position >= d
        before = before + jnp.where(ok, scaled(pieces[d][0], before_log), 0.0)
        before_log = before_log + jnp.where(ok, pieces[d][1], 0.0)
    inside = (scaled(before, inside[1]) + inside[0], inside[1] + before_log)
    group_state = jnp.zeros_like(before)
    for d in range(count):
        later = jnp.zeros_like(before_log)
        for k in range(count):
            if k != d:
                later = later + jnp.where(places[k] > places[d], pieces[k][1], 0.0)
        group_state = group_state + scaled(pieces[d][0], later)
    return inside, pack_state(group_state, sum(piece[1] for piece in pieces))


def tables(rows):
    offset = lax.axis_index(EP) * rows
    position = (offset + jnp.arange(rows, dtype=jnp.int32)).astype(F32)
    inverse = 1.0 / 10000.0 ** jnp.linspace(0.0, 1.0, 32, dtype=F32)
    angles = position[:, None] * jnp.tile(inverse, 4)[None, :]
    sign = jnp.where(jnp.arange(128) % 64 < 32, -1.0, 1.0).astype(F32)
    return jnp.cos(angles), jnp.sin(angles) * sign[None, :]


def running(log_decay):
    heads, rows = log_decay.shape
    chunks = rows // CHUNK
    upper = (jnp.arange(CHUNK)[:, None] <= jnp.arange(CHUNK)[None, :]).astype(F32)
    cum = jnp.dot(
        log_decay.reshape(heads * chunks, CHUNK), upper, precision=lax.Precision.HIGHEST
    ).reshape(heads, chunks, CHUNK)
    return cum.transpose(1, 0, 2), cum.transpose(1, 2, 0).reshape(rows, heads)


def ring_first(value):
    return send(value, "tp", 1), send(value, "tp", -1)


def ring_second(left, right, *earlier):
    half = left.shape[0] // 2
    top, bottom = after(left[:half], *earlier), after(right[half:], *earlier)
    top = send(top, "tp", 1)
    bottom = send(bottom, "tp", -1)
    return [top, bottom]


def project_kernel(place_ref, own, left, top, bottom, right, w_ref, out_ref):
    height = own.shape[1]
    step = pl.program_id(0)
    cross = jnp.where(step < pl.num_programs(0) // 2, top[...], bottom[...])
    total = None
    for d, piece in enumerate((own[...], left[...], cross, right[...])):
        start = pl.multiple_of(((place_ref[0] - d) & 3) * height, height)
        product = mm(piece, w_ref[pl.ds(start, height), :])
        total = product if total is None else total + product
    out_ref[...] = total.astype(BF16)


def projected(place, own, left, top, bottom, right, out_weight):
    rows, width = own.shape
    cols = out_weight.shape[1]
    step = rows // 4
    whole = pl.BlockSpec((step, width), lambda i: (i, 0))
    return pl.pallas_call(
        project_kernel,
        name="projected",
        grid=(4,),
        in_specs=[
            pl.BlockSpec(memory_space=pltpu.SMEM),
            whole,
            whole,
            pl.BlockSpec((step, width), lambda i: (jnp.minimum(i, 1), 0)),
            pl.BlockSpec((step, width), lambda i: (jnp.maximum(i - 2, 0), 0)),
            whole,
            pl.BlockSpec(out_weight.shape, lambda i: (0, 0)),
        ],
        out_specs=pl.BlockSpec((step, cols), lambda i: (i, 0)),
        out_shape=jax.ShapeDtypeStruct((rows, cols), BF16),
        cost_estimate=pl.CostEstimate(
            flops=8 * rows * width * cols, bytes_accessed=10 << 20, transcendentals=0
        ),
    )(place, own, left, top, bottom, right, out_weight)


def token_kernel(x_ref, gain_ref, routes_ref, weights_ref, a_ref, b_ref, meta_ref, *, capacity):
    tokens, width = x_ref.shape
    x = x_ref[...].astype(F32)
    centered = x - jnp.mean(x, axis=1, keepdims=True)
    variance = jnp.mean(centered * centered, axis=1, keepdims=True)
    normed = (centered * lax.rsqrt(variance + 1e-05) * gain_ref[...]).astype(BF16)
    first = routes_ref[0:1, :]
    second = routes_ref[1:2, :]
    expert = lax.broadcasted_iota(jnp.int32, (32, tokens), 0)
    hit_0 = (expert == first).astype(F32)
    hit_1 = (expert == second).astype(F32)
    sooner = lax.broadcasted_iota(jnp.int32, (tokens, tokens), 0) < lax.broadcasted_iota(
        jnp.int32, (tokens, tokens), 1
    )
    earlier = mm((hit_0 + hit_1).astype(BF16), sooner.astype(F32).astype(BF16))
    slot_0 = jnp.sum(earlier * hit_0, axis=0, keepdims=True)
    slot_1 = jnp.sum(earlier * hit_1, axis=0, keepdims=True)
    first_f = first.astype(F32)
    second_f = second.astype(F32)
    row_0 = first_f * ROW + slot_0
    row_1 = second_f * ROW + slot_1
    line = lax.broadcasted_iota(jnp.int32, (8, tokens), 0)
    facts = jnp.zeros((8, tokens), F32)
    for index, row in enumerate(
        (
            first_f * capacity + slot_0,
            second_f * capacity + slot_1,
            weights_ref[0:1, :],
            weights_ref[1:2, :],
            row_0,
            row_1,
        )
    ):
        facts = jnp.where(line == index, row, facts)
    spot = lax.broadcasted_iota(jnp.int32, (8, META), 0) == lax.broadcasted_iota(
        jnp.int32, (8, META), 1
    )
    meta = mm_t(facts.astype(BF16), spot.astype(F32).astype(BF16))
    meta_ref[...] = meta
    place = lax.broadcasted_iota(jnp.int32, (a_ref.shape[0], tokens), 0)
    chosen = jnp.logical_or(
        place == row_0.astype(jnp.int32), place == row_1.astype(jnp.int32)
    )
    a_width = a_ref.shape[1]
    a_ref[...] = mm(chosen.astype(F32).astype(BF16), normed[:, :a_width]).astype(BF16)
    b_ref[:, : width - a_width] = normed[:, a_width:]
    b_ref[:, width - a_width :] = meta.astype(BF16)


def token_rows(expert_input, norm_gain, routes, route_weights, capacity, b_width):
    tokens, width = expert_input.shape
    kernel = lambda *refs: token_kernel(*refs, capacity=float(capacity))
    return pl.pallas_call(
        kernel,
        name="token_rows",
        out_shape=(
            jax.ShapeDtypeStruct((32 * ROW, width - b_width), BF16),
            jax.ShapeDtypeStruct((tokens, b_width + META), BF16),
            jax.ShapeDtypeStruct((tokens, META), F32),
        ),
        cost_estimate=pl.CostEstimate(
            flops=1 << 24, bytes_accessed=1 << 20, transcendentals=tokens
        ),
    )(expert_input, norm_gain[None, :], routes.T, route_weights.T)


def slot_row(target, source_x, source_core, here, capacity):
    expert = (target * 10923) >> 16
    slot = target - expert * capacity
    far = ((expert >> 3) - here[0]) & 3
    near = (((expert >> 1) & 3) - here[1]) & 3
    other = (expert - here[2]) & 1
    row = (far * 4 + near) * 8 * capacity + source_x * 2 * capacity + source_core * capacity + slot
    return jnp.where(other == 0, row, -1)


def place_kernel(here_ref, p0, p1, p2, p3, sw, o0, o1, o2, o3, meta_ref, all_ref, *, capacity):
    tokens = p0.shape[0]
    width = o0.shape[1]
    for d, p in enumerate((p0, p1, p2, p3)):
        all_ref[tokens * d : tokens * d + tokens, :] = p[...]
    all_ref[4 * tokens :, :] = sw[...]
    meta = all_ref[:, width:]
    meta_ref[...] = meta
    here = (here_ref[0], here_ref[1], here_ref[2])
    spot = lax.broadcasted_iota(jnp.int32, (8, META), 0) == lax.broadcasted_iota(
        jnp.int32, (8, META), 1
    )
    facts = lax.dot_general(
        spot.astype(F32).astype(BF16), meta, (((1,), (1,)), ((), ())), preferred_element_type=F32
    )
    token = lax.broadcasted_iota(jnp.int32, (1, 8 * tokens), 1)
    source_core = token // (4 * tokens)
    source_x = token // tokens - 4 * source_core
    rows = [
        slot_row(facts[r : r + 1, :].astype(jnp.int32), source_x, source_core, here, capacity)
        for r in range(2)
    ]
    count = o0.shape[0]
    values = all_ref[:, :width]
    for d, out in enumerate((o0, o1, o2, o3)):
        place = lax.broadcasted_iota(jnp.int32, (count, 8 * tokens), 0) + d * count
        chosen = jnp.logical_or(place == rows[0], place == rows[1])
        out[...] = mm(chosen.astype(F32).astype(BF16), values).astype(BF16)


def placed_rows(here, pieces, swapped, width, capacity):
    tokens = pieces[0].shape[0]
    count = 32 * capacity
    vmem = pl.BlockSpec(memory_space=pltpu.VMEM)
    kernel = lambda *refs: place_kernel(*refs, capacity=capacity)
    result = pl.pallas_call(
        kernel,
        name="placed_rows",
        in_specs=[pl.BlockSpec(memory_space=pltpu.SMEM)] + [vmem] * 5,
        out_specs=(vmem,) * 5,
        out_shape=(jax.ShapeDtypeStruct((count, width), BF16),) * 4
        + (jax.ShapeDtypeStruct((8 * tokens, META), BF16),),
        scratch_shapes=[pltpu.VMEM((8 * tokens, width + META), BF16)],
        cost_estimate=pl.CostEstimate(flops=1 << 30, bytes_accessed=4 << 20, transcendentals=0),
    )(here, *pieces, swapped)
    return list(result[:4]), result[4]


def regroup_kernel(i0, i1, i2, i3, o0, o1, o2, o3):
    count = i0.shape[0] // 4
    for d, out in enumerate((o0, o1, o2, o3)):
        for j, source in enumerate((i0, i1, i2, i3)):
            out[count * j : count * j + count, :] = source[count * d : count * d + count, :]


def regrouped(blocks):
    vmem = pl.BlockSpec(memory_space=pltpu.VMEM)
    shape = jax.ShapeDtypeStruct(blocks[0].shape, BF16)
    return list(
        pl.pallas_call(
            regroup_kernel,
            name="regrouped",
            in_specs=[vmem] * 4,
            out_specs=(vmem,) * 4,
            out_shape=(shape,) * 4,
            cost_estimate=pl.CostEstimate(flops=1 << 20, bytes_accessed=4 << 20, transcendentals=0),
        )(*blocks)
    )


def swap_matrix(side, unit):
    row = lax.broadcasted_iota(jnp.int32, (side, side), 0)
    lane = lax.broadcasted_iota(jnp.int32, (side, side), 1)
    block = 4 * unit
    outer = row // block
    middle = (row - outer * block) // unit
    inside = row - outer * block - middle * unit
    return (lane == middle * block + outer * unit + inside).astype(F32).astype(BF16)


def turn_kernel(i0, i1, i2, i3, out_ref, *, unit):
    side = i0.shape[0]
    block = 4 * unit
    swap = swap_matrix(side, unit)
    for z in range(4):
        part = jnp.concatenate(
            [piece[block * z : block * z + block, :] for piece in (i0, i1, i2, i3)], axis=0
        )
        turned_part = mm(swap, part).astype(BF16)
        for x in range(4):
            out_ref[side * x + block * z : side * x + block * z + block, :] = turned_part[
                block * x : block * x + block, :
            ]


def turned_rows(pieces, unit):
    rows, width = pieces[0].shape
    vmem = pl.BlockSpec(memory_space=pltpu.VMEM)
    return pl.pallas_call(
        lambda *refs: turn_kernel(*refs, unit=unit),
        name="turned_rows",
        in_specs=[vmem] * 4,
        out_specs=vmem,
        out_shape=jax.ShapeDtypeStruct((4 * rows, width), BF16),
        cost_estimate=pl.CostEstimate(flops=1 << 29, bytes_accessed=4 << 20, transcendentals=0),
    )(*pieces)


def back_b_kernel(hidden_ref, w_ref, o0, o1, o2, o3, swapped_ref, *, unit):
    side = hidden_ref.shape[0] // 4
    block = 4 * unit
    swap = swap_matrix(side, unit)
    for z in range(4):
        part = jnp.concatenate(
            [hidden_ref[side * x + block * z : side * x + block * z + block, :] for x in range(4)],
            axis=0,
        )
        turned_part = mm(swap, part).astype(BF16)
        for y in range(4):
            swapped_ref[side * y + block * z : side * y + block * z + block, :] = turned_part[
                block * y : block * y + block, :
            ]
    for y, out in enumerate((o0, o1, o2, o3)):
        out[...] = mm(swapped_ref[side * y : side * y + side, :], w_ref[...]).astype(BF16)


def back_b_rows(hidden, weight, unit):
    rows, inner = hidden.shape
    vmem = pl.BlockSpec(memory_space=pltpu.VMEM)
    shape = jax.ShapeDtypeStruct((rows // 4, R_B), BF16)
    first = (weight.shape[1] - R_B) // R_B
    return list(
        pl.pallas_call(
            lambda *refs: back_b_kernel(*refs, unit=unit),
            name="back_b_rows",
            grid=(1,),
            in_specs=[
                pl.BlockSpec((rows, inner), lambda i: (0, 0)),
                pl.BlockSpec((inner, R_B), lambda i: (0, first)),
            ],
            out_specs=(pl.BlockSpec((rows // 4, R_B), lambda i: (0, 0)),) * 4,
            out_shape=(shape,) * 4,
            scratch_shapes=[pltpu.VMEM((rows, inner), BF16)],
            cost_estimate=pl.CostEstimate(
                flops=1 << 30, bytes_accessed=3 << 20, transcendentals=0
            ),
        )(hidden, weight)
    )


def back_a_rows(hidden, weight, width, spans):
    rows, inner = hidden.shape

    def kernel(hidden_ref, w_ref, *out_refs):
        for (low, high), out in zip(spans, out_refs):
            out[...] = mm(hidden_ref[low:high, :], w_ref[...]).astype(BF16)

    return pl.pallas_call(
        kernel,
        grid=(width // 512,),
        in_specs=[
            pl.BlockSpec((rows, inner), lambda i: (0, 0)),
            pl.BlockSpec((inner, 512), lambda i: (0, i)),
        ],
        out_specs=tuple(pl.BlockSpec((h - l, 512), lambda i: (0, i)) for l, h in spans),
        out_shape=tuple(jax.ShapeDtypeStruct((h - l, width), BF16) for l, h in spans),
        cost_estimate=pl.CostEstimate(flops=2 << 30, bytes_accessed=6 << 20, transcendentals=0),
    )(hidden, weight)


def combine_kernel(here_ref, h0, h1, h2, h3, meta_ref, own_ref, other_ref, *, capacity):
    here = (here_ref[0], here_ref[1], here_ref[2])
    source_core = pl.program_id(0)
    total = meta_ref.shape[0]
    source_x = lax.broadcasted_iota(jnp.int32, (total, 1), 0) // (total // 4)
    meta = meta_ref[...].astype(F32)
    rows = [
        slot_row(meta[:, r : r + 1].astype(jnp.int32), source_x, source_core, here, capacity)
        for r in range(2)
    ]
    count = h0.shape[0]
    result = None
    for d, h in enumerate((h0, h1, h2, h3)):
        place = lax.broadcasted_iota(jnp.int32, (total, count), 1) + d * count
        shares = jnp.where(place == rows[0], meta[:, 2:3], 0.0) + jnp.where(
            place == rows[1], meta[:, 3:4], 0.0
        )
        product = mm(shares.astype(BF16), h[...])
        result = product if result is None else result + product

    @pl.when(source_core == 0)
    def _():
        own_ref[...] = result.astype(BF16)

    @pl.when(source_core == 1)
    def _():
        other_ref[...] = result.astype(BF16)


def combined_rows(here, pieces, meta, capacity):
    half = meta.shape[0] // 2
    rows, width = pieces[0].shape
    kernel = lambda *refs: combine_kernel(*refs, capacity=capacity)
    shape = jax.ShapeDtypeStruct((half, width), BF16)
    piece = pl.BlockSpec((rows, width), lambda i: (0, 0))
    whole = pl.BlockSpec((half, width), lambda i: (0, 0))
    return pl.pallas_call(
        kernel,
        name="combined_rows",
        grid=(2,),
        in_specs=[pl.BlockSpec(memory_space=pltpu.SMEM)]
        + [piece] * 4
        + [pl.BlockSpec((half, META), lambda i: (i, 0))],
        out_specs=(whole, whole),
        out_shape=(shape, shape),
        cost_estimate=pl.CostEstimate(flops=1 << 30, bytes_accessed=4 << 20, transcendentals=0),
    )(here, *pieces, meta)


def exchange(blocks, axis, sign):
    return [blocks[0]] + [send(blocks[d], axis, sign * d) for d in range(1, len(blocks))]


def rows_of(value, count):
    height = value.shape[0] // count
    return [value[height * d : height * (d + 1)] for d in range(count)]


def compaction(capacity):
    place = [lax.axis_index(name) for name in EP]
    index = jnp.arange(32 * capacity, dtype=jnp.int32)
    slot = index % capacity
    digits = index // capacity
    far = (place[0] - digits // 8) % 4
    near = (place[1] - digits // 2) % 4
    core = (place[2] - digits) % 2
    source = ((far * 4 + near) * 2 + core) * ROW + slot
    lanes = jnp.arange(32 * ROW, dtype=jnp.int32)
    return (source[:, None] == lanes[None, :]).astype(BF16)


def per_device(
    query,
    keys,
    values,
    gate_pre,
    log_decay,
    out_weight,
    expert_input,
    norm_gain,
    routes,
    route_weights,
    w_gate,
    w_up,
    w_down,
):
    heads = log_decay.shape[0]
    tokens, width = expert_input.shape
    top = routes.shape[1]
    capacity = 3 * tokens * top // (2 * lax.axis_size(EP))
    unit = 2 * capacity
    block = 4 * unit
    a_width = width - D_B
    gate_w, up_w, down_w = (w_gate[0], w_up[0], w_down[0])

    placed_a, payload_b, meta_a = token_rows(
        expert_input, norm_gain, routes, route_weights, capacity, D_B
    )
    here = jnp.stack([lax.axis_index(name) for name in EP]).astype(jnp.int32)
    got_b = exchange([payload_b] * 4, "tp", 1)
    got_a = lax.all_to_all(placed_a.reshape(32, ROW, a_width), EP, 0, 0, tiled=False)

    held_b = jnp.concatenate(got_b, axis=0)
    other_b = send(held_b, "ep_2", 1)
    decay = after(log_decay, placed_a)
    cosine, sine = tables(query.shape[0])
    cum_c, cum_t = running(decay)
    blocks_b, meta_b = placed_rows(here, got_b, after(other_b, sine), D_B, capacity)
    got_b = exchange(blocks_b, "ep_0", 1)

    state = local_state(after(keys, blocks_b[0]), values, cosine, sine, cum_t)
    inside, group = core_prefix(state, jnp.sum(decay, axis=1))
    inside, group_z = ring_prefix(inside, group, "ep_1", heads)

    compact = compaction(capacity)
    slots_a = mm(compact, after(got_a, group).reshape(32 * ROW, a_width)).astype(BF16)
    left_a, right_a = ring_first(slots_a)
    inside, _ = ring_prefix(inside, after(group_z, slots_a), "ep_0", heads)

    turn_b = regrouped(after(got_b, slots_a))
    got_b = exchange(turn_b, "ep_1", 1)
    gated = gated_output(
        query, keys, values, gate_pre, cosine, sine, cum_c, cum_t, after(inside[0], turn_b[0])
    )
    cross_a = ring_second(left_a, right_a, gated)
    left_g, right_g = ring_first(gated)

    turned_b = turned_rows(after(got_b, gated), unit)
    gate_h = mm(turned_b, gate_w[a_width:])
    up_h = mm(turned_b, up_w[a_width:])
    all_a = jnp.concatenate(after([slots_a, left_a, *cross_a, right_a], gate_h), axis=0)
    gate_h = gate_h + mm(all_a, gate_w[:a_width])
    up_h = up_h + mm(all_a, up_w[:a_width])
    hidden = lax.optimization_barrier((jax.nn.silu(gate_h) * up_h).astype(BF16))

    ra = width - R_B
    half = 2 * block
    upper, lower = back_a_rows(
        hidden, down_w, ra, ((8 * block, 10 * block), (10 * block, 12 * block))
    )
    upper = send(upper, "tp", -1)
    lower = send(lower, "tp", 1)
    back_b = back_b_rows(hidden, down_w, unit)
    got_b = exchange(back_b, "ep_1", -1)
    b0, b1, b3 = back_a_rows(
        after(hidden, back_b[0]),
        down_w,
        ra,
        ((0, 4 * block), (4 * block, 8 * block), (12 * block, 16 * block)),
    )
    b1 = jnp.concatenate([b1[:half] + upper, b1[half:]], axis=0)
    b3 = jnp.concatenate([b3[:half], b3[half:] + lower], axis=0)
    up_a, down_a = send(b1, "tp", -1), send(b3, "tp", 1)
    turn_b = regrouped(after(got_b, b1, b3))
    home_b = exchange(turn_b, "ep_0", -1)
    cross_g = ring_second(left_g, right_g, turn_b[0])
    own_b, other_b = combined_rows(here, home_b, meta_b, capacity)
    other_b = send(other_b, "ep_2", 1)
    summed_a = (after(b0, own_b).astype(F32) + up_a.astype(F32) + down_a.astype(F32)).astype(BF16)
    spread_a = mm_t(compact, summed_a).astype(BF16)
    home_a = lax.all_to_all(
        spread_a.reshape(32, ROW, ra), EP, 0, 0, tiled=False
    ).reshape(32 * ROW, ra)
    mixed_b = own_b + after(other_b, spread_a)
    got_b = exchange(rows_of(mixed_b, 4), "tp", -1)
    place = lax.axis_index("tp").astype(jnp.int32)[None]
    mixed = projected(
        place, gated, left_g, *after(cross_g, mixed_b), right_g, out_weight
    )
    final_b = sum(p.astype(F32) for p in got_b)
    slot_lane = jnp.arange(32 * ROW, dtype=jnp.int32)[None, :]
    shares = sum(
        jnp.where(meta_a[:, 4 + r : 5 + r].astype(jnp.int32) == slot_lane, meta_a[:, 2 + r : 3 + r], 0.0)
        for r in range(top)
    ).astype(BF16)
    final_a = mm(shares, after(home_a, mixed))
    moe_out = jnp.concatenate([final_a, final_b], axis=1).astype(BF16)
    return (mixed, moe_out)


def solution(mesh):
    torus = Mesh(mesh.devices.reshape(4, 4, 2, mesh.shape["tp"]), ("ep_0", "ep_1", "ep_2", "tp"))
    return jax.shard_map(
        per_device,
        mesh=torus,
        in_specs=(
            P(EP, "tp"),
            P(EP, "tp"),
            P(EP, "tp"),
            P(EP, "tp"),
            P("tp", EP),
            P(None, "tp"),
            P(EP_TP, None),
            P(),
            P(EP_TP, None),
            P(EP_TP, None),
            P(EP, None, "tp"),
            P(EP, None, "tp"),
            P(EP, "tp", None),
        ),
        out_specs=(P(EP, "tp"), P(EP_TP, None)),
        check_vma=False,
    )
```

```python
import jax
import jax.numpy as jnp
from jax import lax
from jax.experimental import pallas as pl
from jax.experimental.pallas import tpu as pltpu
from jax.sharding import Mesh
from jax.sharding import PartitionSpec as P


EP = ("ep_0", "ep_1", "ep_2")
EP_TP = ("ep_0", "ep_1", "ep_2", "tp")
CHUNK = 256
META = 128
ROW = 8
D_B = 768
R_B = 1152
F32 = jnp.float32
BF16 = jnp.bfloat16


def send(value, axis, step):
    n = lax.axis_size(axis)
    return lax.ppermute(value, axis, [(i, (i + step) % n) for i in range(n)])


def after(value, *earlier):
    return lax.optimization_barrier((value, earlier))[0]


def mm(a, b):
    return jnp.dot(a, b, preferred_element_type=F32)


def mm_t(a, b):
    return lax.dot_general(a, b, (((0,), (0,)), ((), ())), preferred_element_type=F32)


def turned(x, cosine, sine):
    lane = lax.broadcasted_iota(jnp.int32, x.shape, 1) % 64
    other = jnp.where(lane < 32, pltpu.roll(x, 96, 1), pltpu.roll(x, 32, 1))
    return x * cosine + other * sine


def state_kernel(k_ref, v_ref, cos_ref, sin_ref, cum_t_ref, out_ref, state_ref):
    step = pl.program_id(0)
    heads = v_ref.shape[1] // 128

    @pl.when(step == 0)
    def _():
        state_ref[...] = jnp.zeros_like(state_ref)

    cosine = cos_ref[...]
    sine = sin_ref[...]
    half = lax.broadcasted_iota(jnp.int32, (CHUNK, 128), 1) < 64
    for pair in range(heads // 2):
        lanes = slice(128 * pair, 128 * pair + 128)
        k = turned(k_ref[:, lanes].astype(F32), cosine, sine) * 0.125
        c0 = cum_t_ref[:, 2 * pair : 2 * pair + 1]
        c1 = cum_t_ref[:, 2 * pair + 1 : 2 * pair + 2]
        t0 = c0[CHUNK - 1 : CHUNK, :]
        t1 = c1[CHUNK - 1 : CHUNK, :]
        k = k * jnp.exp(jnp.where(half, t0 - c0, t1 - c1))
        v = v_ref[:, 256 * pair : 256 * pair + 256]
        new = mm_t(k.astype(BF16), v)
        for j, t in ((0, t0), (1, t1)):
            h = 2 * pair + j
            rows = slice(64 * h, 64 * h + 64)
            state_ref[rows, :] = (
                state_ref[rows, :] * jnp.exp(t) + new[64 * j : 64 * j + 64, 128 * j : 128 * j + 128]
            )

    @pl.when(step == pl.num_programs(0) - 1)
    def _():
        out_ref[...] = state_ref[...]


def output_kernel(
    q_ref, k_ref, v_ref, g_ref, cos_ref, sin_ref, cum_ref, cum_t_ref, inc_ref, out_ref, state_ref
):
    step = pl.program_id(0)
    heads = v_ref.shape[1] // 128

    @pl.when(step == 0)
    def _():
        state_ref[...] = jnp.zeros_like(state_ref)
        for h in range(heads):
            low = 64 * (h % 2)
            state_ref[h, low : low + 64, :] = inc_ref[64 * h : 64 * h + 64, :]

    cosine = cos_ref[...]
    sine = sin_ref[...]
    half = lax.broadcasted_iota(jnp.int32, (CHUNK, 128), 1) < 64
    causal = lax.broadcasted_iota(jnp.int32, (CHUNK, CHUNK), 0) >= lax.broadcasted_iota(
        jnp.int32, (CHUNK, CHUNK), 1
    )
    for pair in range(heads // 2):
        lanes = slice(128 * pair, 128 * pair + 128)
        q = turned(q_ref[:, lanes].astype(F32), cosine, sine)
        k = turned(k_ref[:, lanes].astype(F32), cosine, sine) * 0.125
        k_b = k.astype(BF16)
        for j in range(2):
            h = 2 * pair + j
            mine = half if j == 0 else jnp.logical_not(half)
            v = v_ref[:, 128 * h : 128 * h + 128]
            col = cum_t_ref[:, h : h + 1]
            row = cum_ref[0, h : h + 1, :]
            total = col[CHUNK - 1 : CHUNK, :]
            q_h = jnp.where(mine, q, 0.0)
            weights = jnp.exp(jnp.where(causal, col - row, -1e9))
            scores = (
                lax.dot_general(
                    q_h.astype(BF16), k_b, (((1,), (1,)), ((), ())), preferred_element_type=F32
                )
                * weights
            )
            state = state_ref[h]
            out = mm(scores.astype(BF16), v) + mm(
                (q_h * jnp.exp(col)).astype(BF16), state.astype(BF16)
            )
            k_h = jnp.where(mine, k * jnp.exp(total - col), 0.0)
            state_ref[h] = state * jnp.exp(total) + mm_t(k_h.astype(BF16), v)
            centered = out - jnp.mean(out, axis=1, keepdims=True)
            variance = jnp.mean(centered * centered, axis=1, keepdims=True)
            normed = centered * lax.rsqrt(variance + 1e-06)
            gate = g_ref[:, 128 * h : 128 * h + 128].astype(F32)
            out_ref[:, 128 * h : 128 * h + 128] = (gate * jax.nn.sigmoid(gate) * normed).astype(
                BF16
            )


def local_state(keys, values, cosine, sine, cum_t):
    rows, width = keys.shape
    grid = rows // CHUNK
    heads = values.shape[1] // 128
    return pl.pallas_call(
        state_kernel,
        name="local_state",
        grid=(grid,),
        in_specs=[
            pl.BlockSpec((CHUNK, width), lambda i: (i, 0)),
            pl.BlockSpec((CHUNK, values.shape[1]), lambda i: (i, 0)),
            pl.BlockSpec((CHUNK, 128), lambda i: (i, 0)),
            pl.BlockSpec((CHUNK, 128), lambda i: (i, 0)),
            pl.BlockSpec((CHUNK, heads), lambda i: (i, 0)),
        ],
        out_specs=pl.BlockSpec((64 * heads, 128), lambda i: (0, 0)),
        out_shape=jax.ShapeDtypeStruct((64 * heads, 128), F32),
        scratch_shapes=[pltpu.VMEM((64 * heads, 128), F32)],
        cost_estimate=pl.CostEstimate(
            flops=2 * rows * width * 256, bytes_accessed=3 << 20, transcendentals=1 << 18
        ),
    )(keys, values, cosine, sine, cum_t)


def gated_output(query, keys, values, gate_pre, cosine, sine, cum, cum_t, incoming):
    rows, width = keys.shape
    grid = rows // CHUNK
    vw = values.shape[1]
    heads = vw // 128
    return pl.pallas_call(
        output_kernel,
        name="gated_output",
        grid=(grid,),
        in_specs=[
            pl.BlockSpec((CHUNK, width), lambda i: (i, 0)),
            pl.BlockSpec((CHUNK, width), lambda i: (i, 0)),
            pl.BlockSpec((CHUNK, vw), lambda i: (i, 0)),
            pl.BlockSpec((CHUNK, vw), lambda i: (i, 0)),
            pl.BlockSpec((CHUNK, 128), lambda i: (i, 0)),
            pl.BlockSpec((CHUNK, 128), lambda i: (i, 0)),
            pl.BlockSpec((1, heads, CHUNK), lambda i: (i, 0, 0)),
            pl.BlockSpec((CHUNK, heads), lambda i: (i, 0)),
            pl.BlockSpec((64 * heads, 128), lambda i: (0, 0)),
        ],
        out_specs=pl.BlockSpec((CHUNK, vw), lambda i: (i, 0)),
        out_shape=jax.ShapeDtypeStruct((rows, vw), BF16),
        scratch_shapes=[pltpu.VMEM((heads, 128, 128), F32)],
        cost_estimate=pl.CostEstimate(
            flops=10 * 1000 * 1000 * 1000, bytes_accessed=5 << 20, transcendentals=1 << 20
        ),
    )(query, keys, values, gate_pre, cosine, sine, cum, cum_t, incoming)


def pack_state(state, log_total):
    high = log_total.astype(BF16)
    low = (log_total - high.astype(F32)).astype(BF16)
    extra = jnp.concatenate([high[:, None], low[:, None]], axis=0)
    extra = jnp.broadcast_to(extra, (extra.shape[0], 128))
    return jnp.concatenate([state.astype(BF16), extra], axis=0)


def unpack_state(packed, heads):
    state = packed[: 64 * heads].astype(F32)
    logs = packed[64 * heads :, 0].astype(F32)
    return state, logs[:heads] + logs[heads:]


def scaled(state, log_factor):
    return state * jnp.repeat(jnp.exp(log_factor), 64)[:, None]


def core_prefix(state, log_total):
    heads = log_total.shape[0]
    second = lax.axis_index("ep_2") == 1
    mine = pack_state(state, log_total)
    other_state, other_log = unpack_state(send(mine, "ep_2", 1), heads)
    state = unpack_state(mine, heads)[0]
    inside = (jnp.where(second, other_state, 0.0), jnp.where(second, other_log, 0.0))
    first_s = jnp.where(second, other_state, state)
    second_s = jnp.where(second, state, other_state)
    second_log = jnp.where(second, log_total, other_log)
    group = pack_state(scaled(first_s, second_log) + second_s, log_total + other_log)
    return inside, group


def ring_prefix(inside, packed, axis, heads):
    count = lax.axis_size(axis)
    position = lax.axis_index(axis)
    pieces = [unpack_state(packed, heads)] + [
        unpack_state(send(packed, axis, d), heads) for d in range(1, count)
    ]
    places = [(position - d) % count for d in range(count)]
    before = jnp.zeros_like(pieces[0][0])
    before_log = jnp.zeros_like(pieces[0][1])
    for d in range(1, count):
        ok = position >= d
        before = before + jnp.where(ok, scaled(pieces[d][0], before_log), 0.0)
        before_log = before_log + jnp.where(ok, pieces[d][1], 0.0)
    inside = (scaled(before, inside[1]) + inside[0], inside[1] + before_log)
    group_state = jnp.zeros_like(before)
    for d in range(count):
        later = jnp.zeros_like(before_log)
        for k in range(count):
            if k != d:
                later = later + jnp.where(places[k] > places[d], pieces[k][1], 0.0)
        group_state = group_state + scaled(pieces[d][0], later)
    return inside, pack_state(group_state, sum(piece[1] for piece in pieces))


def tables(rows):
    offset = lax.axis_index(EP) * rows
    position = (offset + jnp.arange(rows, dtype=jnp.int32)).astype(F32)
    inverse = 1.0 / 10000.0 ** jnp.linspace(0.0, 1.0, 32, dtype=F32)
    angles = position[:, None] * jnp.tile(inverse, 4)[None, :]
    sign = jnp.where(jnp.arange(128) % 64 < 32, -1.0, 1.0).astype(F32)
    return jnp.cos(angles), jnp.sin(angles) * sign[None, :]


def running(log_decay):
    heads, rows = log_decay.shape
    chunks = rows // CHUNK
    upper = (jnp.arange(CHUNK)[:, None] <= jnp.arange(CHUNK)[None, :]).astype(F32)
    cum = jnp.dot(
        log_decay.reshape(heads * chunks, CHUNK), upper, precision=lax.Precision.HIGHEST
    ).reshape(heads, chunks, CHUNK)
    return cum.transpose(1, 0, 2), cum.transpose(1, 2, 0).reshape(rows, heads)


def ring_first(value):
    return send(value, "tp", 1), send(value, "tp", -1)


def ring_second(left, right, *earlier):
    half = left.shape[0] // 2
    top, bottom = after(left[:half], *earlier), after(right[half:], *earlier)
    top = send(top, "tp", 1)
    bottom = send(bottom, "tp", -1)
    return [top, bottom]


def weight_rows(w_ref, place_ref, d, height):
    start = pl.multiple_of(((place_ref[0] - d) & 3) * height, height)
    return w_ref[pl.ds(start, height), :]


def project_kernel(place_ref, own, left, right, w_ref, out_ref):
    height = own.shape[1]
    total = None
    for d, piece in ((0, own), (1, left), (3, right)):
        product = mm(piece[...], weight_rows(w_ref, place_ref, d, height))
        total = product if total is None else total + product
    out_ref[...] = total


def finish_kernel(place_ref, part_ref, top, bottom, w_ref, out_ref):
    height = top.shape[1]
    step = pl.program_id(0)
    cross = jnp.where(step < pl.num_programs(0) // 2, top[...], bottom[...])
    out_ref[...] = (
        part_ref[...] + mm(cross, weight_rows(w_ref, place_ref, 2, height))
    ).astype(BF16)


def projected(place, own, left, right, out_weight):
    rows, width = own.shape
    cols = out_weight.shape[1]
    step = rows // 4
    whole = pl.BlockSpec((step, width), lambda i: (i, 0))
    return pl.pallas_call(
        project_kernel,
        name="projected",
        grid=(4,),
        in_specs=[pl.BlockSpec(memory_space=pltpu.SMEM)]
        + [whole] * 3
        + [pl.BlockSpec(memory_space=pltpu.VMEM)],
        out_specs=pl.BlockSpec((step, cols), lambda i: (i, 0)),
        out_shape=jax.ShapeDtypeStruct((rows, cols), F32),
        cost_estimate=pl.CostEstimate(
            flops=6 * rows * width * cols, bytes_accessed=10 << 20, transcendentals=0
        ),
    )(place, own, left, right, out_weight)


def finished(place, part, top, bottom, out_weight):
    rows, cols = part.shape
    width = top.shape[1]
    step = rows // 4
    return pl.pallas_call(
        finish_kernel,
        name="finished",
        grid=(4,),
        in_specs=[
            pl.BlockSpec(memory_space=pltpu.SMEM),
            pl.BlockSpec((step, cols), lambda i: (i, 0)),
            pl.BlockSpec((step, width), lambda i: (jnp.minimum(i, 1), 0)),
            pl.BlockSpec((step, width), lambda i: (jnp.maximum(i - 2, 0), 0)),
            pl.BlockSpec(memory_space=pltpu.VMEM),
        ],
        out_specs=pl.BlockSpec((step, cols), lambda i: (i, 0)),
        out_shape=jax.ShapeDtypeStruct((rows, cols), BF16),
        cost_estimate=pl.CostEstimate(
            flops=2 * rows * width * cols, bytes_accessed=10 << 20, transcendentals=0
        ),
    )(place, part, top, bottom, out_weight)


def token_kernel(x_ref, gain_ref, routes_ref, weights_ref, a_ref, b_ref, meta_ref, *, capacity):
    tokens, width = x_ref.shape
    x = x_ref[...].astype(F32)
    centered = x - jnp.mean(x, axis=1, keepdims=True)
    variance = jnp.mean(centered * centered, axis=1, keepdims=True)
    normed = (centered * lax.rsqrt(variance + 1e-05) * gain_ref[...]).astype(BF16)
    first = routes_ref[0:1, :]
    second = routes_ref[1:2, :]
    expert = lax.broadcasted_iota(jnp.int32, (32, tokens), 0)
    hit_0 = (expert == first).astype(F32)
    hit_1 = (expert == second).astype(F32)
    sooner = lax.broadcasted_iota(jnp.int32, (tokens, tokens), 0) < lax.broadcasted_iota(
        jnp.int32, (tokens, tokens), 1
    )
    earlier = mm((hit_0 + hit_1).astype(BF16), sooner.astype(F32).astype(BF16))
    slot_0 = jnp.sum(earlier * hit_0, axis=0, keepdims=True)
    slot_1 = jnp.sum(earlier * hit_1, axis=0, keepdims=True)
    first_f = first.astype(F32)
    second_f = second.astype(F32)
    row_0 = first_f * ROW + slot_0
    row_1 = second_f * ROW + slot_1
    line = lax.broadcasted_iota(jnp.int32, (8, tokens), 0)
    facts = jnp.zeros((8, tokens), F32)
    for index, row in enumerate(
        (
            first_f * capacity + slot_0,
            second_f * capacity + slot_1,
            weights_ref[0:1, :],
            weights_ref[1:2, :],
            row_0,
            row_1,
        )
    ):
        facts = jnp.where(line == index, row, facts)
    spot = lax.broadcasted_iota(jnp.int32, (8, META), 0) == lax.broadcasted_iota(
        jnp.int32, (8, META), 1
    )
    meta = mm_t(facts.astype(BF16), spot.astype(F32).astype(BF16))
    meta_ref[...] = meta
    place = lax.broadcasted_iota(jnp.int32, (a_ref.shape[0], tokens), 0)
    chosen = jnp.logical_or(
        place == row_0.astype(jnp.int32), place == row_1.astype(jnp.int32)
    )
    a_width = a_ref.shape[1]
    a_ref[...] = mm(chosen.astype(F32).astype(BF16), normed[:, :a_width]).astype(BF16)
    b_ref[:, : width - a_width] = normed[:, a_width:]
    b_ref[:, width - a_width :] = meta.astype(BF16)


def token_rows(expert_input, norm_gain, routes, route_weights, capacity, b_width):
    tokens, width = expert_input.shape
    kernel = lambda *refs: token_kernel(*refs, capacity=float(capacity))
    return pl.pallas_call(
        kernel,
        name="token_rows",
        out_shape=(
            jax.ShapeDtypeStruct((32 * ROW, width - b_width), BF16),
            jax.ShapeDtypeStruct((tokens, b_width + META), BF16),
            jax.ShapeDtypeStruct((tokens, META), F32),
        ),
        cost_estimate=pl.CostEstimate(
            flops=1 << 24, bytes_accessed=1 << 20, transcendentals=tokens
        ),
    )(expert_input, norm_gain[None, :], routes.T, route_weights.T)


def slot_row(target, source_x, source_core, here, capacity):
    expert = (target * 10923) >> 16
    slot = target - expert * capacity
    far = ((expert >> 3) - here[0]) & 3
    near = (((expert >> 1) & 3) - here[1]) & 3
    other = (expert - here[2]) & 1
    row = (far * 4 + near) * 8 * capacity + source_x * 2 * capacity + source_core * capacity + slot
    return jnp.where(other == 0, row, -1)


def place_kernel(here_ref, p0, p1, p2, p3, sw, o0, o1, o2, o3, meta_ref, all_ref, *, capacity):
    tokens = p0.shape[0]
    width = o0.shape[1]
    for d, p in enumerate((p0, p1, p2, p3)):
        all_ref[tokens * d : tokens * d + tokens, :] = p[...]
    all_ref[4 * tokens :, :] = sw[...]
    meta = all_ref[:, width:]
    meta_ref[...] = meta
    here = (here_ref[0], here_ref[1], here_ref[2])
    spot = lax.broadcasted_iota(jnp.int32, (8, META), 0) == lax.broadcasted_iota(
        jnp.int32, (8, META), 1
    )
    facts = lax.dot_general(
        spot.astype(F32).astype(BF16), meta, (((1,), (1,)), ((), ())), preferred_element_type=F32
    )
    token = lax.broadcasted_iota(jnp.int32, (1, 8 * tokens), 1)
    source_core = token // (4 * tokens)
    source_x = token // tokens - 4 * source_core
    rows = [
        slot_row(facts[r : r + 1, :].astype(jnp.int32), source_x, source_core, here, capacity)
        for r in range(2)
    ]
    count = o0.shape[0]
    values = all_ref[:, :width]
    for d, out in enumerate((o0, o1, o2, o3)):
        place = lax.broadcasted_iota(jnp.int32, (count, 8 * tokens), 0) + d * count
        chosen = jnp.logical_or(place == rows[0], place == rows[1])
        out[...] = mm(chosen.astype(F32).astype(BF16), values).astype(BF16)


def placed_rows(here, pieces, swapped, width, capacity):
    tokens = pieces[0].shape[0]
    count = 32 * capacity
    vmem = pl.BlockSpec(memory_space=pltpu.VMEM)
    kernel = lambda *refs: place_kernel(*refs, capacity=capacity)
    result = pl.pallas_call(
        kernel,
        name="placed_rows",
        in_specs=[pl.BlockSpec(memory_space=pltpu.SMEM)] + [vmem] * 5,
        out_specs=(vmem,) * 5,
        out_shape=(jax.ShapeDtypeStruct((count, width), BF16),) * 4
        + (jax.ShapeDtypeStruct((8 * tokens, META), BF16),),
        scratch_shapes=[pltpu.VMEM((8 * tokens, width + META), BF16)],
        cost_estimate=pl.CostEstimate(flops=1 << 30, bytes_accessed=4 << 20, transcendentals=0),
    )(here, *pieces, swapped)
    return list(result[:4]), result[4]


def regroup_kernel(i0, i1, i2, i3, o0, o1, o2, o3):
    count = i0.shape[0] // 4
    for d, out in enumerate((o0, o1, o2, o3)):
        for j, source in enumerate((i0, i1, i2, i3)):
            out[count * j : count * j + count, :] = source[count * d : count * d + count, :]


def regrouped(blocks):
    vmem = pl.BlockSpec(memory_space=pltpu.VMEM)
    shape = jax.ShapeDtypeStruct(blocks[0].shape, BF16)
    return list(
        pl.pallas_call(
            regroup_kernel,
            name="regrouped",
            in_specs=[vmem] * 4,
            out_specs=(vmem,) * 4,
            out_shape=(shape,) * 4,
            cost_estimate=pl.CostEstimate(flops=1 << 20, bytes_accessed=4 << 20, transcendentals=0),
        )(*blocks)
    )


def swap_matrix(side, unit):
    row = lax.broadcasted_iota(jnp.int32, (side, side), 0)
    lane = lax.broadcasted_iota(jnp.int32, (side, side), 1)
    block = 4 * unit
    outer = row // block
    middle = (row - outer * block) // unit
    inside = row - outer * block - middle * unit
    return (lane == middle * block + outer * unit + inside).astype(F32).astype(BF16)


def turn_kernel(i0, i1, i2, i3, out_ref, *, unit):
    side = i0.shape[0]
    block = 4 * unit
    swap = swap_matrix(side, unit)
    for z in range(4):
        part = jnp.concatenate(
            [piece[block * z : block * z + block, :] for piece in (i0, i1, i2, i3)], axis=0
        )
        turned_part = mm(swap, part).astype(BF16)
        for x in range(4):
            out_ref[side * x + block * z : side * x + block * z + block, :] = turned_part[
                block * x : block * x + block, :
            ]


def turned_rows(pieces, unit):
    rows, width = pieces[0].shape
    vmem = pl.BlockSpec(memory_space=pltpu.VMEM)
    return pl.pallas_call(
        lambda *refs: turn_kernel(*refs, unit=unit),
        name="turned_rows",
        in_specs=[vmem] * 4,
        out_specs=vmem,
        out_shape=jax.ShapeDtypeStruct((4 * rows, width), BF16),
        cost_estimate=pl.CostEstimate(flops=1 << 29, bytes_accessed=4 << 20, transcendentals=0),
    )(*pieces)


def near_kernel(first, second, third, gate_ref, up_ref, gate_out, up_out, rows_ref):
    side, width = first.shape
    for place, piece in enumerate((first, second, third)):
        rows_ref[side * place : side * place + side, :] = piece[...]
    rows = rows_ref[...]
    gate_out[...] = mm(rows, gate_ref[:width, :])
    up_out[...] = mm(rows, up_ref[:width, :])


def near_sums(pieces, gate_w, up_w):
    side, width = pieces[0].shape
    inner = gate_w.shape[1]
    vmem = pl.BlockSpec(memory_space=pltpu.VMEM)
    return pl.pallas_call(
        near_kernel,
        name="near_sums",
        in_specs=[vmem] * 5,
        out_specs=(vmem, vmem),
        out_shape=(jax.ShapeDtypeStruct((3 * side, inner), F32),) * 2,
        scratch_shapes=[pltpu.VMEM((3 * side, width), BF16)],
        cost_estimate=pl.CostEstimate(
            flops=12 * side * width * inner, bytes_accessed=12 << 20, transcendentals=0
        ),
    )(*pieces, gate_w, up_w)


def hidden_kernel(top, bottom, b_ref, gate_sum, up_sum, gate_ref, up_ref, near_ref, far_ref):
    half, width = top.shape
    side = 2 * half
    far = jnp.concatenate([top[...], bottom[...]], axis=0)
    b_rows = b_ref[...]
    gate_b = mm(b_rows, gate_ref[width:, :])
    up_b = mm(b_rows, up_ref[width:, :])
    gate_far = mm(far, gate_ref[:width, :]) + gate_b[2 * side : 3 * side]
    up_far = mm(far, up_ref[:width, :]) + up_b[2 * side : 3 * side]
    far_ref[...] = (gate_far * jax.nn.sigmoid(gate_far) * up_far).astype(BF16)
    for place, x in enumerate((0, 1, 3)):
        low = side * place
        gate = gate_sum[low : low + side, :] + gate_b[side * x : side * x + side]
        up = up_sum[low : low + side, :] + up_b[side * x : side * x + side]
        near_ref[low : low + side, :] = (gate * jax.nn.sigmoid(gate) * up).astype(BF16)


def hidden_rows(cross, b_rows, sums, gate_w, up_w):
    half = cross[0].shape[0]
    width, inner = gate_w.shape
    vmem = pl.BlockSpec(memory_space=pltpu.VMEM)
    return pl.pallas_call(
        hidden_kernel,
        name="hidden_rows",
        in_specs=[vmem] * 7,
        out_specs=(vmem, vmem),
        out_shape=(
            jax.ShapeDtypeStruct((6 * half, inner), BF16),
            jax.ShapeDtypeStruct((2 * half, inner), BF16),
        ),
        cost_estimate=pl.CostEstimate(
            flops=16 * half * width * inner, bytes_accessed=12 << 20, transcendentals=8 * half * inner
        ),
    )(*cross, b_rows, *sums, gate_w, up_w)


def back_b_kernel(near_ref, far_ref, w_ref, o0, o1, o2, o3, swapped_ref, *, unit):
    side = far_ref.shape[0]
    block = 4 * unit
    swap = swap_matrix(side, unit)
    for z in range(4):
        low = block * z
        part = jnp.concatenate(
            [
                near_ref[low : low + block, :],
                near_ref[side + low : side + low + block, :],
                far_ref[low : low + block, :],
                near_ref[2 * side + low : 2 * side + low + block, :],
            ],
            axis=0,
        )
        turned_part = mm(swap, part).astype(BF16)
        for y in range(4):
            swapped_ref[side * y + low : side * y + low + block, :] = turned_part[
                block * y : block * y + block, :
            ]
    result = mm(swapped_ref[...], w_ref[:, w_ref.shape[1] - o0.shape[1] :]).astype(BF16)
    for y, out in enumerate((o0, o1, o2, o3)):
        out[...] = result[side * y : side * y + side, :]


def back_b_rows(near, far, weight, unit):
    side, inner = far.shape
    vmem = pl.BlockSpec(memory_space=pltpu.VMEM)
    shape = jax.ShapeDtypeStruct((side, R_B), BF16)
    return list(
        pl.pallas_call(
            lambda *refs: back_b_kernel(*refs, unit=unit),
            name="back_b_rows",
            in_specs=[vmem] * 3,
            out_specs=(vmem,) * 4,
            out_shape=(shape,) * 4,
            scratch_shapes=[pltpu.VMEM((4 * side, inner), BF16)],
            cost_estimate=pl.CostEstimate(
                flops=1 << 30, bytes_accessed=3 << 20, transcendentals=0
            ),
        )(near, far, weight)
    )


def back_a_rows(hidden, weight, width, spans):
    vmem = pl.BlockSpec(memory_space=pltpu.VMEM)

    def kernel(hidden_ref, w_ref, *out_refs):
        result = mm(hidden_ref[...], w_ref[:, :width]).astype(BF16)
        for (low, high), out in zip(spans, out_refs):
            out[...] = result[low:high, :]

    return pl.pallas_call(
        kernel,
        in_specs=[vmem] * 2,
        out_specs=(vmem,) * len(spans),
        out_shape=tuple(jax.ShapeDtypeStruct((h - l, width), BF16) for l, h in spans),
        cost_estimate=pl.CostEstimate(flops=2 << 30, bytes_accessed=6 << 20, transcendentals=0),
    )(hidden, weight)


def combine_kernel(here_ref, h0, h1, h2, h3, meta_ref, own_ref, other_ref, *, capacity):
    here = (here_ref[0], here_ref[1], here_ref[2])
    source_core = pl.program_id(0)
    total = meta_ref.shape[0]
    source_x = lax.broadcasted_iota(jnp.int32, (total, 1), 0) // (total // 4)
    meta = meta_ref[...].astype(F32)
    rows = [
        slot_row(meta[:, r : r + 1].astype(jnp.int32), source_x, source_core, here, capacity)
        for r in range(2)
    ]
    count = h0.shape[0]
    result = None
    for d, h in enumerate((h0, h1, h2, h3)):
        place = lax.broadcasted_iota(jnp.int32, (total, count), 1) + d * count
        shares = jnp.where(place == rows[0], meta[:, 2:3], 0.0) + jnp.where(
            place == rows[1], meta[:, 3:4], 0.0
        )
        product = mm(shares.astype(BF16), h[...])
        result = product if result is None else result + product

    @pl.when(source_core == 0)
    def _():
        own_ref[...] = result.astype(BF16)

    @pl.when(source_core == 1)
    def _():
        other_ref[...] = result.astype(BF16)


def combined_rows(here, pieces, meta, capacity):
    half = meta.shape[0] // 2
    rows, width = pieces[0].shape
    kernel = lambda *refs: combine_kernel(*refs, capacity=capacity)
    shape = jax.ShapeDtypeStruct((half, width), BF16)
    piece = pl.BlockSpec((rows, width), lambda i: (0, 0))
    whole = pl.BlockSpec((half, width), lambda i: (0, 0))
    return pl.pallas_call(
        kernel,
        name="combined_rows",
        grid=(2,),
        in_specs=[pl.BlockSpec(memory_space=pltpu.SMEM)]
        + [piece] * 4
        + [pl.BlockSpec((half, META), lambda i: (i, 0))],
        out_specs=(whole, whole),
        out_shape=(shape, shape),
        cost_estimate=pl.CostEstimate(flops=1 << 30, bytes_accessed=4 << 20, transcendentals=0),
    )(here, *pieces, meta)


def exchange(blocks, axis, sign):
    return [blocks[0]] + [send(blocks[d], axis, sign * d) for d in range(1, len(blocks))]


def rows_of(value, count):
    height = value.shape[0] // count
    return [value[height * d : height * (d + 1)] for d in range(count)]


def compaction(capacity):
    place = [lax.axis_index(name) for name in EP]
    index = jnp.arange(32 * capacity, dtype=jnp.int32)
    slot = index % capacity
    digits = index // capacity
    far = (place[0] - digits // 8) % 4
    near = (place[1] - digits // 2) % 4
    core = (place[2] - digits) % 2
    source = ((far * 4 + near) * 2 + core) * ROW + slot
    lanes = jnp.arange(32 * ROW, dtype=jnp.int32)
    return (source[:, None] == lanes[None, :]).astype(BF16)


def per_device(
    query,
    keys,
    values,
    gate_pre,
    log_decay,
    out_weight,
    expert_input,
    norm_gain,
    routes,
    route_weights,
    w_gate,
    w_up,
    w_down,
):
    heads = log_decay.shape[0]
    tokens, width = expert_input.shape
    top = routes.shape[1]
    capacity = 3 * tokens * top // (2 * lax.axis_size(EP))
    unit = 2 * capacity
    block = 4 * unit
    a_width = width - D_B
    gate_w, up_w, down_w = (w_gate[0], w_up[0], w_down[0])

    placed_a, payload_b, meta_a = token_rows(
        expert_input, norm_gain, routes, route_weights, capacity, D_B
    )
    here = jnp.stack([lax.axis_index(name) for name in EP]).astype(jnp.int32)
    got_b = exchange([payload_b] * 4, "tp", 1)
    got_a = lax.all_to_all(placed_a.reshape(32, ROW, a_width), EP, 0, 0, tiled=False)

    held_b = jnp.concatenate(got_b, axis=0)
    other_b = send(held_b, "ep_2", 1)
    decay = after(log_decay, placed_a)
    cosine, sine = tables(query.shape[0])
    cum_c, cum_t = running(decay)

    state = local_state(after(keys, sine), values, cosine, sine, cum_t)
    inside, group = core_prefix(state, jnp.sum(decay, axis=1))
    inside, group_z = ring_prefix(inside, group, "ep_1", heads)
    blocks_b, meta_b = placed_rows(here, got_b, after(other_b, group), D_B, capacity)

    compact = compaction(capacity)
    slots_a = mm(
        compact, after(got_a, blocks_b[0]).reshape(32 * ROW, a_width)
    ).astype(BF16)
    left_a, right_a = ring_first(slots_a)
    inside, _ = ring_prefix(inside, after(group_z, slots_a), "ep_0", heads)
    got_b = exchange(blocks_b, "ep_0", 1)

    gated = gated_output(
        query, keys, values, gate_pre, cosine, sine, cum_c, cum_t, inside[0]
    )
    turn_b = regrouped(after(got_b, gated))
    got_b = exchange(turn_b, "ep_1", 1)
    cross_a = ring_second(left_a, right_a, turn_b[0])
    left_g, right_g = ring_first(gated)

    side = 4 * block
    sums = near_sums([slots_a, left_a, right_a], gate_w, up_w)
    turned_b = turned_rows(after(got_b, sums), unit)
    near, far = hidden_rows(after(cross_a, turned_b), turned_b, sums, gate_w, up_w)

    ra = width - R_B
    half = 2 * block
    upper, lower = back_a_rows(far, down_w, ra, ((0, half), (half, side)))
    upper = send(upper, "tp", -1)
    lower = send(lower, "tp", 1)
    back_b = back_b_rows(near, far, down_w, unit)
    got_b = exchange(back_b, "ep_1", -1)
    b0, b1, b3 = back_a_rows(
        after(near, back_b[0]), down_w, ra, ((0, side), (side, 2 * side), (2 * side, 3 * side))
    )
    b1 = jnp.concatenate([b1[:half] + upper, b1[half:]], axis=0)
    b3 = jnp.concatenate([b3[:half], b3[half:] + lower], axis=0)
    up_a, down_a = send(b1, "tp", -1), send(b3, "tp", 1)
    place = lax.axis_index("tp").astype(jnp.int32)[None]
    part = projected(place, after(gated, b1, b3), left_g, right_g, out_weight)
    turn_b = regrouped(after(got_b, part))
    home_b = exchange(turn_b, "ep_0", -1)
    cross_g = ring_second(left_g, right_g, turn_b[0])
    summed_a = (
        after(b0, turn_b[0]).astype(F32) + up_a.astype(F32) + down_a.astype(F32)
    ).astype(BF16)
    spread_a = mm_t(compact, summed_a).astype(BF16)
    home_a = lax.all_to_all(
        spread_a.reshape(32, ROW, ra), EP, 0, 0, tiled=False
    ).reshape(32 * ROW, ra)
    facts_a = after(meta_a, spread_a)
    slot_lane = jnp.arange(32 * ROW, dtype=jnp.int32)[None, :]
    shares = sum(
        jnp.where(facts_a[:, 4 + r : 5 + r].astype(jnp.int32) == slot_lane, facts_a[:, 2 + r : 3 + r], 0.0)
        for r in range(top)
    ).astype(BF16)
    own_b, other_b = combined_rows(here, after(home_b, spread_a), meta_b, capacity)
    other_b = send(other_b, "ep_2", 1)
    mixed_b = own_b + other_b
    got_b = exchange(rows_of(mixed_b, 4), "tp", -1)
    mixed = finished(place, part, *after(cross_g, mixed_b), out_weight)
    final_b = sum(p.astype(F32) for p in got_b)
    final_a = mm(shares, after(home_a, mixed))
    moe_out = jnp.concatenate([final_a, final_b], axis=1).astype(BF16)
    return (mixed, moe_out)


def solution(mesh):
    torus = Mesh(mesh.devices.reshape(4, 4, 2, mesh.shape["tp"]), ("ep_0", "ep_1", "ep_2", "tp"))
    return jax.shard_map(
        per_device,
        mesh=torus,
        in_specs=(
            P(EP, "tp"),
            P(EP, "tp"),
            P(EP, "tp"),
            P(EP, "tp"),
            P("tp", EP),
            P(None, "tp"),
            P(EP_TP, None),
            P(),
            P(EP_TP, None),
            P(EP_TP, None),
            P(EP, None, "tp"),
            P(EP, None, "tp"),
            P(EP, "tp", None),
        ),
        out_specs=(P(EP, "tp"), P(EP_TP, None)),
        check_vma=False,
    )
```

```python
import jax
import jax.numpy as jnp
from jax import lax
from jax.experimental import pallas as pl
from jax.experimental.pallas import tpu as pltpu
from jax.sharding import Mesh
from jax.sharding import PartitionSpec as P


Z, Y, C, X = "ep_0", "ep_1", "ep_2", "tp"
EP = (Z, Y, C)
EP_TP = (Z, Y, C, X)
CHUNK = 256
META = 128
ROW = 8
D_B = 768
R_B = 1152
F32 = jnp.float32
BF16 = jnp.bfloat16


def send(value, axis, step):
    n = lax.axis_size(axis)
    return lax.ppermute(value, axis, [(i, (i + step) % n) for i in range(n)])


def after(value, *earlier):
    return lax.optimization_barrier((value, earlier))[0]


def mm(a, b):
    return jnp.dot(a, b, preferred_element_type=F32)


def mm_t(a, b):
    return lax.dot_general(a, b, (((0,), (0,)), ((), ())), preferred_element_type=F32)


def turned(x, cosine, sine):
    lane = lax.broadcasted_iota(jnp.int32, x.shape, 1) % 64
    other = jnp.where(lane < 32, pltpu.roll(x, 96, 1), pltpu.roll(x, 32, 1))
    return x * cosine + other * sine


def state_kernel(k_ref, v_ref, cos_ref, sin_ref, cum_t_ref, out_ref, state_ref):
    step = pl.program_id(0)
    heads = v_ref.shape[1] // 128

    @pl.when(step == 0)
    def _():
        state_ref[...] = jnp.zeros_like(state_ref)

    cosine = cos_ref[...]
    sine = sin_ref[...]
    half = lax.broadcasted_iota(jnp.int32, (CHUNK, 128), 1) < 64
    for pair in range(heads // 2):
        lanes = slice(128 * pair, 128 * pair + 128)
        k = turned(k_ref[:, lanes].astype(F32), cosine, sine) * 0.125
        c0 = cum_t_ref[:, 2 * pair : 2 * pair + 1]
        c1 = cum_t_ref[:, 2 * pair + 1 : 2 * pair + 2]
        t0 = c0[CHUNK - 1 : CHUNK, :]
        t1 = c1[CHUNK - 1 : CHUNK, :]
        k = k * jnp.exp(jnp.where(half, t0 - c0, t1 - c1))
        v = v_ref[:, 256 * pair : 256 * pair + 256]
        new = mm_t(k.astype(BF16), v)
        for j, t in ((0, t0), (1, t1)):
            h = 2 * pair + j
            rows = slice(64 * h, 64 * h + 64)
            state_ref[rows, :] = (
                state_ref[rows, :] * jnp.exp(t) + new[64 * j : 64 * j + 64, 128 * j : 128 * j + 128]
            )

    @pl.when(step == pl.num_programs(0) - 1)
    def _():
        out_ref[...] = state_ref[...]


def output_kernel(
    q_ref, k_ref, v_ref, g_ref, cos_ref, sin_ref, cum_ref, cum_t_ref, inc_ref, out_ref, state_ref
):
    step = pl.program_id(0)
    heads = v_ref.shape[1] // 128

    @pl.when(step == 0)
    def _():
        state_ref[...] = jnp.zeros_like(state_ref)
        for h in range(heads):
            low = 64 * (h % 2)
            state_ref[h, low : low + 64, :] = inc_ref[64 * h : 64 * h + 64, :]

    cosine = cos_ref[...]
    sine = sin_ref[...]
    half = lax.broadcasted_iota(jnp.int32, (CHUNK, 128), 1) < 64
    causal = lax.broadcasted_iota(jnp.int32, (CHUNK, CHUNK), 0) >= lax.broadcasted_iota(
        jnp.int32, (CHUNK, CHUNK), 1
    )
    for pair in range(heads // 2):
        lanes = slice(128 * pair, 128 * pair + 128)
        q = turned(q_ref[:, lanes].astype(F32), cosine, sine)
        k = turned(k_ref[:, lanes].astype(F32), cosine, sine) * 0.125
        k_b = k.astype(BF16)
        for j in range(2):
            h = 2 * pair + j
            mine = half if j == 0 else jnp.logical_not(half)
            v = v_ref[:, 128 * h : 128 * h + 128]
            col = cum_t_ref[:, h : h + 1]
            row = cum_ref[0, h : h + 1, :]
            total = col[CHUNK - 1 : CHUNK, :]
            q_h = jnp.where(mine, q, 0.0)
            weights = jnp.exp(jnp.where(causal, col - row, -1e9))
            scores = (
                lax.dot_general(
                    q_h.astype(BF16), k_b, (((1,), (1,)), ((), ())), preferred_element_type=F32
                )
                * weights
            )
            state = state_ref[h]
            out = mm(scores.astype(BF16), v) + mm(
                (q_h * jnp.exp(col)).astype(BF16), state.astype(BF16)
            )
            k_h = jnp.where(mine, k * jnp.exp(total - col), 0.0)
            state_ref[h] = state * jnp.exp(total) + mm_t(k_h.astype(BF16), v)
            centered = out - jnp.mean(out, axis=1, keepdims=True)
            variance = jnp.mean(centered * centered, axis=1, keepdims=True)
            normed = centered * lax.rsqrt(variance + 1e-06)
            gate = g_ref[:, 128 * h : 128 * h + 128].astype(F32)
            out_ref[:, 128 * h : 128 * h + 128] = (gate * jax.nn.sigmoid(gate) * normed).astype(
                BF16
            )


def local_state(keys, values, cosine, sine, cum_t):
    rows, width = keys.shape
    grid = rows // CHUNK
    heads = values.shape[1] // 128
    return pl.pallas_call(
        state_kernel,
        name="local_state",
        grid=(grid,),
        in_specs=[
            pl.BlockSpec((CHUNK, width), lambda i: (i, 0)),
            pl.BlockSpec((CHUNK, values.shape[1]), lambda i: (i, 0)),
            pl.BlockSpec((CHUNK, 128), lambda i: (i, 0)),
            pl.BlockSpec((CHUNK, 128), lambda i: (i, 0)),
            pl.BlockSpec((CHUNK, heads), lambda i: (i, 0)),
        ],
        out_specs=pl.BlockSpec((64 * heads, 128), lambda i: (0, 0)),
        out_shape=jax.ShapeDtypeStruct((64 * heads, 128), F32),
        scratch_shapes=[pltpu.VMEM((64 * heads, 128), F32)],
        cost_estimate=pl.CostEstimate(
            flops=2 * rows * width * 256, bytes_accessed=3 << 20, transcendentals=1 << 18
        ),
    )(keys, values, cosine, sine, cum_t)


def gated_output(query, keys, values, gate_pre, cosine, sine, cum, cum_t, incoming):
    rows, width = keys.shape
    grid = rows // CHUNK
    vw = values.shape[1]
    heads = vw // 128
    return pl.pallas_call(
        output_kernel,
        name="gated_output",
        grid=(grid,),
        in_specs=[
            pl.BlockSpec((CHUNK, width), lambda i: (i, 0)),
            pl.BlockSpec((CHUNK, width), lambda i: (i, 0)),
            pl.BlockSpec((CHUNK, vw), lambda i: (i, 0)),
            pl.BlockSpec((CHUNK, vw), lambda i: (i, 0)),
            pl.BlockSpec((CHUNK, 128), lambda i: (i, 0)),
            pl.BlockSpec((CHUNK, 128), lambda i: (i, 0)),
            pl.BlockSpec((1, heads, CHUNK), lambda i: (i, 0, 0)),
            pl.BlockSpec((CHUNK, heads), lambda i: (i, 0)),
            pl.BlockSpec((64 * heads, 128), lambda i: (0, 0)),
        ],
        out_specs=pl.BlockSpec((CHUNK, vw), lambda i: (i, 0)),
        out_shape=jax.ShapeDtypeStruct((rows, vw), BF16),
        scratch_shapes=[pltpu.VMEM((heads, 128, 128), F32)],
        cost_estimate=pl.CostEstimate(
            flops=10 * 1000 * 1000 * 1000, bytes_accessed=5 << 20, transcendentals=1 << 20
        ),
    )(query, keys, values, gate_pre, cosine, sine, cum, cum_t, incoming)


def pack_state(state, log_total):
    high = log_total.astype(BF16)
    low = (log_total - high.astype(F32)).astype(BF16)
    extra = jnp.concatenate([high[:, None], low[:, None]], axis=0)
    extra = jnp.broadcast_to(extra, (extra.shape[0], 128))
    return jnp.concatenate([state.astype(BF16), extra], axis=0)


def unpack_state(packed, heads):
    state = packed[: 64 * heads].astype(F32)
    logs = packed[64 * heads :, 0].astype(F32)
    return state, logs[:heads] + logs[heads:]


def scaled(state, log_factor):
    return state * jnp.repeat(jnp.exp(log_factor), 64)[:, None]


def core_prefix(state, log_total):
    heads = log_total.shape[0]
    second = lax.axis_index(C) == 1
    mine = pack_state(state, log_total)
    other_state, other_log = unpack_state(send(mine, C, 1), heads)
    state = unpack_state(mine, heads)[0]
    inside = (jnp.where(second, other_state, 0.0), jnp.where(second, other_log, 0.0))
    first_s = jnp.where(second, other_state, state)
    second_s = jnp.where(second, state, other_state)
    second_log = jnp.where(second, log_total, other_log)
    group = pack_state(scaled(first_s, second_log) + second_s, log_total + other_log)
    return inside, group


def ring_prefix(inside, packed, axis, heads):
    count = lax.axis_size(axis)
    position = lax.axis_index(axis)
    pieces = [unpack_state(packed, heads)] + [
        unpack_state(send(packed, axis, d), heads) for d in range(1, count)
    ]
    places = [(position - d) % count for d in range(count)]
    before = jnp.zeros_like(pieces[0][0])
    before_log = jnp.zeros_like(pieces[0][1])
    for d in range(1, count):
        ok = position >= d
        before = before + jnp.where(ok, scaled(pieces[d][0], before_log), 0.0)
        before_log = before_log + jnp.where(ok, pieces[d][1], 0.0)
    inside = (scaled(before, inside[1]) + inside[0], inside[1] + before_log)
    group_state = jnp.zeros_like(before)
    for d in range(count):
        later = jnp.zeros_like(before_log)
        for k in range(count):
            if k != d:
                later = later + jnp.where(places[k] > places[d], pieces[k][1], 0.0)
        group_state = group_state + scaled(pieces[d][0], later)
    return inside, pack_state(group_state, sum(piece[1] for piece in pieces))


def tables(rows):
    offset = lax.axis_index(EP) * rows
    position = (offset + jnp.arange(rows, dtype=jnp.int32)).astype(F32)
    inverse = 1.0 / 10000.0 ** jnp.linspace(0.0, 1.0, 32, dtype=F32)
    angles = position[:, None] * jnp.tile(inverse, 4)[None, :]
    sign = jnp.where(jnp.arange(128) % 64 < 32, -1.0, 1.0).astype(F32)
    return jnp.cos(angles), jnp.sin(angles) * sign[None, :]


def running(log_decay):
    heads, rows = log_decay.shape
    chunks = rows // CHUNK
    upper = (jnp.arange(CHUNK)[:, None] <= jnp.arange(CHUNK)[None, :]).astype(F32)
    cum = jnp.dot(
        log_decay.reshape(heads * chunks, CHUNK), upper, precision=lax.Precision.HIGHEST
    ).reshape(heads, chunks, CHUNK)
    return cum.transpose(1, 0, 2), cum.transpose(1, 2, 0).reshape(rows, heads)


def ring_first(value):
    return send(value, X, 1), send(value, X, -1)


def ring_second(left, right, *earlier):
    half = left.shape[0] // 2
    top, bottom = after(left[:half], *earlier), after(right[half:], *earlier)
    top = send(top, X, 1)
    bottom = send(bottom, X, -1)
    return [top, bottom]


def weight_rows(w_ref, place_ref, d, height):
    start = pl.multiple_of(((place_ref[0] - d) & 3) * height, height)
    return w_ref[pl.ds(start, height), :]


def project_kernel(place_ref, own, left, right, w_ref, out_ref):
    height = own.shape[1]
    total = None
    for d, piece in ((0, own), (1, left), (3, right)):
        product = mm(piece[...], weight_rows(w_ref, place_ref, d, height))
        total = product if total is None else total + product
    out_ref[...] = total


def finish_kernel(place_ref, part_ref, top, bottom, w_ref, out_ref):
    height = top.shape[1]
    step = pl.program_id(0)
    cross = jnp.where(step < pl.num_programs(0) // 2, top[...], bottom[...])
    out_ref[...] = (
        part_ref[...] + mm(cross, weight_rows(w_ref, place_ref, 2, height))
    ).astype(BF16)


def projected(place, own, left, right, out_weight):
    rows, width = own.shape
    cols = out_weight.shape[1]
    step = rows // 4
    whole = pl.BlockSpec((step, width), lambda i: (i, 0))
    return pl.pallas_call(
        project_kernel,
        name="projected",
        grid=(4,),
        in_specs=[pl.BlockSpec(memory_space=pltpu.SMEM)]
        + [whole] * 3
        + [pl.BlockSpec(memory_space=pltpu.VMEM)],
        out_specs=pl.BlockSpec((step, cols), lambda i: (i, 0)),
        out_shape=jax.ShapeDtypeStruct((rows, cols), F32),
        cost_estimate=pl.CostEstimate(
            flops=6 * rows * width * cols, bytes_accessed=10 << 20, transcendentals=0
        ),
    )(place, own, left, right, out_weight)


def finished(place, part, top, bottom, out_weight):
    rows, cols = part.shape
    width = top.shape[1]
    step = rows // 4
    return pl.pallas_call(
        finish_kernel,
        name="finished",
        grid=(4,),
        in_specs=[
            pl.BlockSpec(memory_space=pltpu.SMEM),
            pl.BlockSpec((step, cols), lambda i: (i, 0)),
            pl.BlockSpec((step, width), lambda i: (jnp.minimum(i, 1), 0)),
            pl.BlockSpec((step, width), lambda i: (jnp.maximum(i - 2, 0), 0)),
            pl.BlockSpec(memory_space=pltpu.VMEM),
        ],
        out_specs=pl.BlockSpec((step, cols), lambda i: (i, 0)),
        out_shape=jax.ShapeDtypeStruct((rows, cols), BF16),
        cost_estimate=pl.CostEstimate(
            flops=2 * rows * width * cols, bytes_accessed=10 << 20, transcendentals=0
        ),
    )(place, part, top, bottom, out_weight)


def token_kernel(x_ref, gain_ref, routes_ref, weights_ref, a_ref, b_ref, meta_ref, *, capacity):
    tokens, width = x_ref.shape
    x = x_ref[...].astype(F32)
    centered = x - jnp.mean(x, axis=1, keepdims=True)
    variance = jnp.mean(centered * centered, axis=1, keepdims=True)
    normed = (centered * lax.rsqrt(variance + 1e-05) * gain_ref[...]).astype(BF16)
    first = routes_ref[0:1, :]
    second = routes_ref[1:2, :]
    expert = lax.broadcasted_iota(jnp.int32, (32, tokens), 0)
    hit_0 = (expert == first).astype(F32)
    hit_1 = (expert == second).astype(F32)
    sooner = lax.broadcasted_iota(jnp.int32, (tokens, tokens), 0) < lax.broadcasted_iota(
        jnp.int32, (tokens, tokens), 1
    )
    earlier = mm((hit_0 + hit_1).astype(BF16), sooner.astype(F32).astype(BF16))
    slot_0 = jnp.sum(earlier * hit_0, axis=0, keepdims=True)
    slot_1 = jnp.sum(earlier * hit_1, axis=0, keepdims=True)
    first_f = first.astype(F32)
    second_f = second.astype(F32)
    row_0 = first_f * ROW + slot_0
    row_1 = second_f * ROW + slot_1
    line = lax.broadcasted_iota(jnp.int32, (8, tokens), 0)
    facts = jnp.zeros((8, tokens), F32)
    for index, row in enumerate(
        (
            first_f * capacity + slot_0,
            second_f * capacity + slot_1,
            weights_ref[0:1, :],
            weights_ref[1:2, :],
            row_0,
            row_1,
        )
    ):
        facts = jnp.where(line == index, row, facts)
    spot = lax.broadcasted_iota(jnp.int32, (8, META), 0) == lax.broadcasted_iota(
        jnp.int32, (8, META), 1
    )
    meta = mm_t(facts.astype(BF16), spot.astype(F32).astype(BF16))
    meta_ref[...] = meta
    place = lax.broadcasted_iota(jnp.int32, (a_ref.shape[0], tokens), 0)
    chosen = jnp.logical_or(
        place == row_0.astype(jnp.int32), place == row_1.astype(jnp.int32)
    )
    a_width = a_ref.shape[1]
    a_ref[...] = mm(chosen.astype(F32).astype(BF16), normed[:, :a_width]).astype(BF16)
    b_ref[:, : width - a_width] = normed[:, a_width:]
    b_ref[:, width - a_width :] = meta.astype(BF16)


def token_rows(expert_input, norm_gain, routes, route_weights, capacity, b_width):
    tokens, width = expert_input.shape
    kernel = lambda *refs: token_kernel(*refs, capacity=float(capacity))
    return pl.pallas_call(
        kernel,
        name="token_rows",
        out_shape=(
            jax.ShapeDtypeStruct((32 * ROW, width - b_width), BF16),
            jax.ShapeDtypeStruct((tokens, b_width + META), BF16),
            jax.ShapeDtypeStruct((tokens, META), F32),
        ),
        cost_estimate=pl.CostEstimate(
            flops=1 << 24, bytes_accessed=1 << 20, transcendentals=tokens
        ),
    )(expert_input, norm_gain[None, :], routes.T, route_weights.T)


def slot_row(target, source_x, source_core, here, capacity):
    expert = (target * 10923) >> 16
    slot = target - expert * capacity
    far = ((expert >> 3) - here[0]) & 3
    near = (((expert >> 1) & 3) - here[1]) & 3
    other = (expert - here[2]) & 1
    row = (far * 4 + near) * 8 * capacity + source_x * 2 * capacity + source_core * capacity + slot
    return jnp.where(other == 0, row, -1)


def place_kernel(here_ref, p0, p1, p2, p3, sw, o0, o1, o2, o3, meta_ref, all_ref, *, capacity):
    tokens = p0.shape[0]
    width = o0.shape[1]
    for d, p in enumerate((p0, p1, p2, p3)):
        all_ref[tokens * d : tokens * d + tokens, :] = p[...]
    all_ref[4 * tokens :, :] = sw[...]
    meta = all_ref[:, width:]
    meta_ref[...] = meta
    here = (here_ref[0], here_ref[1], here_ref[2])
    spot = lax.broadcasted_iota(jnp.int32, (8, META), 0) == lax.broadcasted_iota(
        jnp.int32, (8, META), 1
    )
    facts = lax.dot_general(
        spot.astype(F32).astype(BF16), meta, (((1,), (1,)), ((), ())), preferred_element_type=F32
    )
    token = lax.broadcasted_iota(jnp.int32, (1, 8 * tokens), 1)
    source_core = token // (4 * tokens)
    source_x = token // tokens - 4 * source_core
    rows = [
        slot_row(facts[r : r + 1, :].astype(jnp.int32), source_x, source_core, here, capacity)
        for r in range(2)
    ]
    count = o0.shape[0]
    values = all_ref[:, :width]
    for d, out in enumerate((o0, o1, o2, o3)):
        place = lax.broadcasted_iota(jnp.int32, (count, 8 * tokens), 0) + d * count
        chosen = jnp.logical_or(place == rows[0], place == rows[1])
        out[...] = mm(chosen.astype(F32).astype(BF16), values).astype(BF16)


def placed_rows(here, pieces, swapped, width, capacity):
    tokens = pieces[0].shape[0]
    count = 32 * capacity
    vmem = pl.BlockSpec(memory_space=pltpu.VMEM)
    kernel = lambda *refs: place_kernel(*refs, capacity=capacity)
    result = pl.pallas_call(
        kernel,
        name="placed_rows",
        in_specs=[pl.BlockSpec(memory_space=pltpu.SMEM)] + [vmem] * 5,
        out_specs=(vmem,) * 5,
        out_shape=(jax.ShapeDtypeStruct((count, width), BF16),) * 4
        + (jax.ShapeDtypeStruct((8 * tokens, META), BF16),),
        scratch_shapes=[pltpu.VMEM((8 * tokens, width + META), BF16)],
        cost_estimate=pl.CostEstimate(flops=1 << 30, bytes_accessed=4 << 20, transcendentals=0),
    )(here, *pieces, swapped)
    return list(result[:4]), result[4]


def regroup_kernel(i0, i1, i2, i3, o0, o1, o2, o3):
    count = i0.shape[0] // 4
    for d, out in enumerate((o0, o1, o2, o3)):
        for j, source in enumerate((i0, i1, i2, i3)):
            out[count * j : count * j + count, :] = source[count * d : count * d + count, :]


def regrouped(blocks):
    vmem = pl.BlockSpec(memory_space=pltpu.VMEM)
    shape = jax.ShapeDtypeStruct(blocks[0].shape, BF16)
    return list(
        pl.pallas_call(
            regroup_kernel,
            name="regrouped",
            in_specs=[vmem] * 4,
            out_specs=(vmem,) * 4,
            out_shape=(shape,) * 4,
            cost_estimate=pl.CostEstimate(flops=1 << 20, bytes_accessed=4 << 20, transcendentals=0),
        )(*blocks)
    )


def swap_matrix(side, unit):
    row = lax.broadcasted_iota(jnp.int32, (side, side), 0)
    lane = lax.broadcasted_iota(jnp.int32, (side, side), 1)
    block = 4 * unit
    outer = row // block
    middle = (row - outer * block) // unit
    inside = row - outer * block - middle * unit
    return (lane == middle * block + outer * unit + inside).astype(F32).astype(BF16)


def turn_kernel(i0, i1, i2, i3, out_ref, *, unit):
    side = i0.shape[0]
    block = 4 * unit
    swap = swap_matrix(side, unit)
    for z in range(4):
        part = jnp.concatenate(
            [piece[block * z : block * z + block, :] for piece in (i0, i1, i2, i3)], axis=0
        )
        turned_part = mm(swap, part).astype(BF16)
        for x in range(4):
            out_ref[side * x + block * z : side * x + block * z + block, :] = turned_part[
                block * x : block * x + block, :
            ]


def turned_rows(pieces, unit):
    rows, width = pieces[0].shape
    vmem = pl.BlockSpec(memory_space=pltpu.VMEM)
    return pl.pallas_call(
        lambda *refs: turn_kernel(*refs, unit=unit),
        name="turned_rows",
        in_specs=[vmem] * 4,
        out_specs=vmem,
        out_shape=jax.ShapeDtypeStruct((4 * rows, width), BF16),
        cost_estimate=pl.CostEstimate(flops=1 << 29, bytes_accessed=4 << 20, transcendentals=0),
    )(*pieces)


def near_kernel(first, second, third, gate_ref, up_ref, gate_out, up_out, rows_ref):
    side, width = first.shape
    for place, piece in enumerate((first, second, third)):
        rows_ref[side * place : side * place + side, :] = piece[...]
    rows = rows_ref[...]
    gate_out[...] = mm(rows, gate_ref[:width, :])
    up_out[...] = mm(rows, up_ref[:width, :])


def near_sums(pieces, gate_w, up_w):
    side, width = pieces[0].shape
    inner = gate_w.shape[1]
    vmem = pl.BlockSpec(memory_space=pltpu.VMEM)
    return pl.pallas_call(
        near_kernel,
        name="near_sums",
        in_specs=[vmem] * 5,
        out_specs=(vmem, vmem),
        out_shape=(jax.ShapeDtypeStruct((3 * side, inner), F32),) * 2,
        scratch_shapes=[pltpu.VMEM((3 * side, width), BF16)],
        cost_estimate=pl.CostEstimate(
            flops=12 * side * width * inner, bytes_accessed=12 << 20, transcendentals=0
        ),
    )(*pieces, gate_w, up_w)


def hidden_kernel(top, bottom, b_ref, gate_sum, up_sum, gate_ref, up_ref, near_ref, far_ref):
    half, width = top.shape
    side = 2 * half
    far = jnp.concatenate([top[...], bottom[...]], axis=0)
    b_rows = b_ref[...]
    gate_b = mm(b_rows, gate_ref[width:, :])
    up_b = mm(b_rows, up_ref[width:, :])
    gate_far = mm(far, gate_ref[:width, :]) + gate_b[2 * side : 3 * side]
    up_far = mm(far, up_ref[:width, :]) + up_b[2 * side : 3 * side]
    far_ref[...] = (gate_far * jax.nn.sigmoid(gate_far) * up_far).astype(BF16)
    for place, x in enumerate((0, 1, 3)):
        low = side * place
        gate = gate_sum[low : low + side, :] + gate_b[side * x : side * x + side]
        up = up_sum[low : low + side, :] + up_b[side * x : side * x + side]
        near_ref[low : low + side, :] = (gate * jax.nn.sigmoid(gate) * up).astype(BF16)


def hidden_rows(cross, b_rows, sums, gate_w, up_w):
    half = cross[0].shape[0]
    width, inner = gate_w.shape
    vmem = pl.BlockSpec(memory_space=pltpu.VMEM)
    return pl.pallas_call(
        hidden_kernel,
        name="hidden_rows",
        in_specs=[vmem] * 7,
        out_specs=(vmem, vmem),
        out_shape=(
            jax.ShapeDtypeStruct((6 * half, inner), BF16),
            jax.ShapeDtypeStruct((2 * half, inner), BF16),
        ),
        cost_estimate=pl.CostEstimate(
            flops=16 * half * width * inner, bytes_accessed=12 << 20, transcendentals=8 * half * inner
        ),
    )(*cross, b_rows, *sums, gate_w, up_w)


def back_b_kernel(near_ref, far_ref, w_ref, o0, o1, o2, o3, swapped_ref, *, unit):
    side = far_ref.shape[0]
    block = 4 * unit
    swap = swap_matrix(side, unit)
    for z in range(4):
        low = block * z
        part = jnp.concatenate(
            [
                near_ref[low : low + block, :],
                near_ref[side + low : side + low + block, :],
                far_ref[low : low + block, :],
                near_ref[2 * side + low : 2 * side + low + block, :],
            ],
            axis=0,
        )
        turned_part = mm(swap, part).astype(BF16)
        for y in range(4):
            swapped_ref[side * y + low : side * y + low + block, :] = turned_part[
                block * y : block * y + block, :
            ]
    result = mm(swapped_ref[...], w_ref[:, w_ref.shape[1] - o0.shape[1] :]).astype(BF16)
    for y, out in enumerate((o0, o1, o2, o3)):
        out[...] = result[side * y : side * y + side, :]


def back_b_rows(near, far, weight, unit):
    side, inner = far.shape
    vmem = pl.BlockSpec(memory_space=pltpu.VMEM)
    shape = jax.ShapeDtypeStruct((side, R_B), BF16)
    return list(
        pl.pallas_call(
            lambda *refs: back_b_kernel(*refs, unit=unit),
            name="back_b_rows",
            in_specs=[vmem] * 3,
            out_specs=(vmem,) * 4,
            out_shape=(shape,) * 4,
            scratch_shapes=[pltpu.VMEM((4 * side, inner), BF16)],
            cost_estimate=pl.CostEstimate(
                flops=1 << 30, bytes_accessed=3 << 20, transcendentals=0
            ),
        )(near, far, weight)
    )


def back_a_rows(hidden, weight, width, spans):
    vmem = pl.BlockSpec(memory_space=pltpu.VMEM)

    def kernel(hidden_ref, w_ref, *out_refs):
        result = mm(hidden_ref[...], w_ref[:, :width]).astype(BF16)
        for (low, high), out in zip(spans, out_refs):
            out[...] = result[low:high, :]

    return pl.pallas_call(
        kernel,
        in_specs=[vmem] * 2,
        out_specs=(vmem,) * len(spans),
        out_shape=tuple(jax.ShapeDtypeStruct((h - l, width), BF16) for l, h in spans),
        cost_estimate=pl.CostEstimate(flops=2 << 30, bytes_accessed=6 << 20, transcendentals=0),
    )(hidden, weight)


def combine_kernel(here_ref, h0, h1, h2, h3, meta_ref, own_ref, other_ref, *, capacity):
    here = (here_ref[0], here_ref[1], here_ref[2])
    source_core = pl.program_id(0)
    total = meta_ref.shape[0]
    source_x = lax.broadcasted_iota(jnp.int32, (total, 1), 0) // (total // 4)
    meta = meta_ref[...].astype(F32)
    rows = [
        slot_row(meta[:, r : r + 1].astype(jnp.int32), source_x, source_core, here, capacity)
        for r in range(2)
    ]
    count = h0.shape[0]
    result = None
    for d, h in enumerate((h0, h1, h2, h3)):
        place = lax.broadcasted_iota(jnp.int32, (total, count), 1) + d * count
        shares = jnp.where(place == rows[0], meta[:, 2:3], 0.0) + jnp.where(
            place == rows[1], meta[:, 3:4], 0.0
        )
        product = mm(shares.astype(BF16), h[...])
        result = product if result is None else result + product

    @pl.when(source_core == 0)
    def _():
        own_ref[...] = result.astype(BF16)

    @pl.when(source_core == 1)
    def _():
        other_ref[...] = result.astype(BF16)


def combined_rows(here, pieces, meta, capacity):
    half = meta.shape[0] // 2
    rows, width = pieces[0].shape
    kernel = lambda *refs: combine_kernel(*refs, capacity=capacity)
    shape = jax.ShapeDtypeStruct((half, width), BF16)
    piece = pl.BlockSpec((rows, width), lambda i: (0, 0))
    whole = pl.BlockSpec((half, width), lambda i: (0, 0))
    return pl.pallas_call(
        kernel,
        name="combined_rows",
        grid=(2,),
        in_specs=[pl.BlockSpec(memory_space=pltpu.SMEM)]
        + [piece] * 4
        + [pl.BlockSpec((half, META), lambda i: (i, 0))],
        out_specs=(whole, whole),
        out_shape=(shape, shape),
        cost_estimate=pl.CostEstimate(flops=1 << 30, bytes_accessed=4 << 20, transcendentals=0),
    )(here, *pieces, meta)


def exchange(blocks, axis, sign):
    return [blocks[0]] + [send(blocks[d], axis, sign * d) for d in range(1, len(blocks))]


def rows_of(value, count):
    height = value.shape[0] // count
    return [value[height * d : height * (d + 1)] for d in range(count)]


def compaction(capacity):
    place = [lax.axis_index(name) for name in EP]
    index = jnp.arange(32 * capacity, dtype=jnp.int32)
    slot = index % capacity
    digits = index // capacity
    far = (place[0] - digits // 8) % 4
    near = (place[1] - digits // 2) % 4
    core = (place[2] - digits) % 2
    source = ((far * 4 + near) * 2 + core) * ROW + slot
    lanes = jnp.arange(32 * ROW, dtype=jnp.int32)
    return (source[:, None] == lanes[None, :]).astype(BF16)


def per_device(
    query,
    keys,
    values,
    gate_pre,
    log_decay,
    out_weight,
    expert_input,
    norm_gain,
    routes,
    route_weights,
    w_gate,
    w_up,
    w_down,
):
    heads = log_decay.shape[0]
    tokens, width = expert_input.shape
    top = routes.shape[1]
    capacity = 3 * tokens * top // (2 * lax.axis_size(EP))
    unit = 2 * capacity
    block = 4 * unit
    a_width = width - D_B
    gate_w, up_w, down_w = (w_gate[0], w_up[0], w_down[0])

    placed_a, payload_b, meta_a = token_rows(
        expert_input, norm_gain, routes, route_weights, capacity, D_B
    )
    here = jnp.stack([lax.axis_index(name) for name in EP]).astype(jnp.int32)
    got_b = exchange([payload_b] * 4, X, 1)
    got_a = lax.all_to_all(placed_a.reshape(32, ROW, a_width), EP, 0, 0, tiled=False)

    held_b = jnp.concatenate(got_b, axis=0)
    other_b = send(held_b, C, 1)
    decay = after(log_decay, placed_a)
    cosine, sine = tables(query.shape[0])
    cum_c, cum_t = running(decay)

    state = local_state(after(keys, sine), values, cosine, sine, cum_t)
    inside, group = core_prefix(state, jnp.sum(decay, axis=1))
    inside, group_z = ring_prefix(inside, group, Y, heads)
    blocks_b, meta_b = placed_rows(here, got_b, after(other_b, group), D_B, capacity)

    compact = compaction(capacity)
    slots_a = mm(
        compact, after(got_a, blocks_b[0]).reshape(32 * ROW, a_width)
    ).astype(BF16)
    left_a, right_a = ring_first(slots_a)
    inside, _ = ring_prefix(inside, after(group_z, slots_a), Z, heads)
    got_b = exchange(blocks_b, Z, 1)

    gated = gated_output(
        query, keys, values, gate_pre, cosine, sine, cum_c, cum_t, inside[0]
    )
    turn_b = regrouped(after(got_b, gated))
    got_b = exchange(turn_b, Y, 1)
    cross_a = ring_second(left_a, right_a, turn_b[0])
    left_g, right_g = ring_first(gated)

    side = 4 * block
    sums = near_sums([slots_a, left_a, right_a], gate_w, up_w)
    turned_b = turned_rows(after(got_b, sums), unit)
    near, far = hidden_rows(after(cross_a, turned_b), turned_b, sums, gate_w, up_w)

    ra = width - R_B
    half = 2 * block
    upper, lower = back_a_rows(far, down_w, ra, ((0, half), (half, side)))
    upper = send(upper, X, -1)
    lower = send(lower, X, 1)
    back_b = back_b_rows(near, far, down_w, unit)
    got_b = exchange(back_b, Y, -1)
    b0, b1, b3 = back_a_rows(
        after(near, back_b[0]), down_w, ra, ((0, side), (side, 2 * side), (2 * side, 3 * side))
    )
    b1 = jnp.concatenate([b1[:half] + upper, b1[half:]], axis=0)
    b3 = jnp.concatenate([b3[:half], b3[half:] + lower], axis=0)
    up_a, down_a = send(b1, X, -1), send(b3, X, 1)
    place = lax.axis_index(X).astype(jnp.int32)[None]
    part = projected(place, after(gated, b1, b3), left_g, right_g, out_weight)
    turn_b = regrouped(after(got_b, part))
    home_b = exchange(turn_b, Z, -1)
    cross_g = ring_second(left_g, right_g, turn_b[0])
    summed_a = (
        after(b0, turn_b[0]).astype(F32) + up_a.astype(F32) + down_a.astype(F32)
    ).astype(BF16)
    spread_a = mm_t(compact, summed_a).astype(BF16)
    home_a = lax.all_to_all(
        spread_a.reshape(32, ROW, ra), EP, 0, 0, tiled=False
    ).reshape(32 * ROW, ra)
    facts_a = after(meta_a, spread_a)
    slot_lane = jnp.arange(32 * ROW, dtype=jnp.int32)[None, :]
    shares = sum(
        jnp.where(facts_a[:, 4 + r : 5 + r].astype(jnp.int32) == slot_lane, facts_a[:, 2 + r : 3 + r], 0.0)
        for r in range(top)
    ).astype(BF16)
    own_b, other_b = combined_rows(here, after(home_b, spread_a), meta_b, capacity)
    other_b = send(other_b, C, 1)
    mixed_b = own_b + other_b
    got_b = exchange(rows_of(mixed_b, 4), X, -1)
    mixed = finished(place, part, *after(cross_g, mixed_b), out_weight)
    final_b = sum(p.astype(F32) for p in got_b)
    final_a = mm(shares, after(home_a, mixed))
    moe_out = jnp.concatenate([final_a, final_b], axis=1).astype(BF16)
    return (mixed, moe_out)


def solution(mesh):
    torus = Mesh(mesh.devices.reshape(4, 4, 2, mesh.shape[X]), EP_TP)
    return jax.shard_map(
        per_device,
        mesh=torus,
        in_specs=(
            P(EP, X),
            P(EP, X),
            P(EP, X),
            P(EP, X),
            P(X, EP),
            P(None, X),
            P(EP_TP, None),
            P(),
            P(EP_TP, None),
            P(EP_TP, None),
            P(EP, None, X),
            P(EP, None, X),
            P(EP, X, None),
        ),
        out_specs=(P(EP, X), P(EP_TP, None)),
        check_vma=False,
    )
```
